32 devices in a mesh: sp: 16 (over z, y, core), dp: 2 (over x).
Axes of the slice: x: 2, y: 2, z: 4, core: 2. Of those that a mesh axis runs over, the one named last changes fastest.
Arguments:
- signal: bfloat16 [2, 2048, 1024], P('dp', 'sp'), may hold values from -6 to 6
- pace: float32 [2, 16], P('dp'), may hold values from 0.5 to 2
- log_step: float32 [64], P('sp'), may hold values from -5.52 to -4.42
- a_real: float32 [64, 64], P('sp'), may hold values from -4 to -0.002, as said below
- a_imag: float32 [64, 64], P('sp'), may hold values from 0.5 to 201.06177
- in_map: float32 [64, 2, 64, 16], P('sp'), may hold values from -3 to 3
- out_map: float32 [64, 2, 16, 64], P('sp'), may hold values from -0.5 to 0.5
- skip: float32 [1024], P('sp'), may hold values from -1 to 1
- init_state: float32 [2, 2, 64, 64], P('dp', None, 'sp'), may hold values from -5 to 5
- w_glu: bfloat16 [1024, 1024], P('sp', 'dp'), may hold values from -0.1875 to 0.1875
- b_glu: float32 [1024], replicated, may hold values from -4 to 4
- g_mix: float32 [1024], replicated, may hold values from 0.1 to 1.9
- w_out: bfloat16 [1024, 4096], P('sp', 'dp'), may hold values from -0.1875 to 0.1875
Outputs:
- result: bfloat16 [2, 2048, 4096], P('dp', 'sp')
The draws below stay inside these ranges and needn't reach their ends.
Inputs may be any that keep to these rules, and one draw needn't show every extreme that they name: `a_real`: negative entries; within a group all entries are of one order.
All inputs are finite; a program needn't handle non-finite values.
Results may differ from the reference program's by a relative error of at most 0.0075.
Values may be sent and summed in bfloat16 or wider, within the bound.
A program may use at most 64 MiB of HBM per device.

```python
import math
import jax
import jax.numpy as jnp
from jax import lax

D = 4096
GROUPS = 64
C = 16
P_SIZE = 64
WIDTH = 1024
LENGTH = 2048
BATCH = 2
SPANS = 16


def draw_a_real(key, part):
    first, second, third = jax.random.split(key, 3)
    share = 0.5
    slow = jax.random.uniform(first, (GROUPS, 1), jnp.float32) < share
    slow_rate = jax.random.uniform(second, (GROUPS, P_SIZE), jnp.float32, 0.002, 0.006)
    fast_rate = jax.random.uniform(third, (GROUPS, P_SIZE), jnp.float32, 1.5, 4.0)
    return -jnp.where(slow, slow_rate, fast_rate)


def block_scale(own_key, extent, pieces, low, high):
    def one(axis_at, shards_of):
        steps = jax.random.uniform(jax.random.fold_in(jax.random.fold_in(own_key, 6), axis_at), (shards_of,), jnp.float32, low / len(pieces), high / len(pieces))
        return jnp.repeat(jnp.exp(steps), extent[axis_at] // shards_of).reshape((-1,) + (1,) * (len(extent) - axis_at - 1))

    level = one(*pieces[0])
    for cut in pieces[1:]:
        level = level * one(*cut)
    return level


def scatter_about(own_key, extent, width, reach, pieces=(), kind=jnp.bfloat16):
    factor_of = block_scale(own_key, extent, pieces, -0.22, 0.18) if pieces else 1.0
    result = jax.random.normal(own_key, extent, jnp.float32) * width * factor_of
    return jnp.minimum(jnp.maximum(result, -reach), reach).astype(kind)


def setup_inputs(seed: int = 0) -> dict:
    seeds = jax.random.split(jax.random.key(seed), 14)
    return {
        "signal": scatter_about(seeds[0], (BATCH, LENGTH, WIDTH), 1.0, 6.0, ((0, 2), (1, 16))),
        "pace": jnp.clip(jnp.exp(math.log(2.0) - 1.3862944 * jax.random.uniform(seeds[1], (BATCH, SPANS), jnp.float32) ** block_scale(seeds[1], (BATCH, SPANS), ((0, 2),), -0.2, 0.2)), 0.5, 2.0),
        "log_step": jnp.clip(-5.52 + 1.0999999 * jax.random.uniform(seeds[2], (GROUPS,), jnp.float32) ** block_scale(seeds[2], (GROUPS,), ((0, 16),), -0.2, 0.2), -5.52, -4.42),
        "a_real": draw_a_real(jax.random.fold_in(seeds[13], 71), 0),
        "a_imag": jnp.clip(0.5 + 200.56177 * jax.random.uniform(seeds[4], (GROUPS, P_SIZE), jnp.float32) ** block_scale(seeds[4], (GROUPS, P_SIZE), ((0, 16),), -0.2, 0.2), 0.5, 201.06177),
        "in_map": scatter_about(seeds[5], (GROUPS, 2, P_SIZE, C), 0.5, 3.0, ((0, 16),), jnp.float32),
        "out_map": scatter_about(seeds[6], (GROUPS, 2, C, P_SIZE), (2 * P_SIZE) ** -0.5, 0.5, ((0, 16),), jnp.float32),
        "skip": jnp.clip(jax.random.uniform(seeds[7], (WIDTH,), jnp.float32, -1.0, 1.0) * block_scale(seeds[7], (WIDTH,), ((0, 16),), -0.4, 0.0), -1.0, 1.0),
        "init_state": scatter_about(seeds[8], (BATCH, 2, GROUPS, P_SIZE), 1.0, 5.0, ((0, 2), (2, 16)), jnp.float32),
        "w_glu": scatter_about(seeds[9], (WIDTH, WIDTH), WIDTH ** -0.5, 0.1875, ((0, 16), (1, 2))),
        "b_glu": scatter_about(seeds[10], (WIDTH,), 1.0, 4.0, (), jnp.float32),
        "g_mix": jnp.clip(1.0 + 0.18 * jax.random.normal(seeds[11], (WIDTH,), jnp.float32), 0.1, 1.9),
        "w_out": scatter_about(seeds[12], (WIDTH, D), WIDTH ** -0.5, 0.1875, ((0, 16), (1, 2))),
    }


def combine(first, second):
    a1r, a1i, b1r, b1i = first
    a2r, a2i, b2r, b2i = second
    return (a2r * a1r - a2i * a1i, a2r * a1i + a2i * a1r, a2r * b1r - a2i * b1i + b2r, a2r * b1i + a2i * b1r + b2i)

def mix_group(series, pace_row, log_rate, a_re, a_im, in_map, out_map, skip_row, init):
    blocks_count = pace_row.shape[0]
    length = series.shape[0]
    span = length // blocks_count
    states = a_re.shape[0]
    steps = (jnp.exp(log_rate) * pace_row)[:, None]
    decay = jnp.exp(a_re * steps)
    bar_re = decay * jnp.cos(a_im * steps)
    bar_im = decay * jnp.sin(a_im * steps)
    modulus = a_re * a_re + a_im * a_im
    coef_re = ((bar_re - 1.0) * a_re + bar_im * a_im) / modulus
    coef_im = (bar_im * a_re - (bar_re - 1.0) * a_im) / modulus
    drive_re = coef_re[..., None] * in_map[0] - coef_im[..., None] * in_map[1]
    drive_im = coef_re[..., None] * in_map[1] + coef_im[..., None] * in_map[0]
    drive = jnp.concatenate([drive_re, drive_im], axis=1).astype(jnp.bfloat16)
    blocks = series.reshape(blocks_count, span, series.shape[1])
    inject = jnp.einsum('ksc,kpc->ksp', blocks.astype(jnp.float32), drive.astype(jnp.float32))
    inject = inject.reshape(length, 2 * states)
    in_re = inject[:, :states]
    in_im = inject[:, states:]
    in_re = in_re.at[0].add(bar_re[0] * init[0] - bar_im[0] * init[1])
    in_im = in_im.at[0].add(bar_re[0] * init[1] + bar_im[0] * init[0])
    step_re = jnp.broadcast_to(bar_re[:, None, :], (blocks_count, span, states)).reshape(length, states)
    step_im = jnp.broadcast_to(bar_im[:, None, :], (blocks_count, span, states)).reshape(length, states)
    scanned = lax.associative_scan(combine, (step_re, step_im, in_re, in_im), axis=0)
    highest = lax.Precision.HIGHEST
    response = jnp.dot(scanned[2], out_map[0].T, precision=highest) - jnp.dot(scanned[3], out_map[1].T, precision=highest)
    response = response + skip_row * series.astype(jnp.float32)
    return jax.nn.gelu(response).astype(jnp.bfloat16)

def reference(signal, pace, log_step, a_real, a_imag, in_map, out_map, skip, init_state, w_glu, b_glu, g_mix, w_out):
    grouped = signal.reshape(BATCH, LENGTH, GROUPS, C)
    skips = skip.reshape(GROUPS, C)

    def per_sequence(index):
        sample = lax.dynamic_index_in_dim(grouped, index, 0, keepdims=False)
        pace_row = lax.dynamic_index_in_dim(pace, index, 0, keepdims=False)
        init_row = lax.dynamic_index_in_dim(init_state, index, 0, keepdims=False)

        def per_group(group):
            series = lax.dynamic_index_in_dim(sample, group, 1, keepdims=False)
            start = lax.dynamic_index_in_dim(init_row, group, 1, keepdims=False)
            return mix_group(series, pace_row, log_step[group], a_real[group], a_imag[group], in_map[group], out_map[group], skips[group], start)
        outputs = lax.map(per_group, jnp.arange(GROUPS, dtype=jnp.int32))
        activated = outputs.transpose(1, 0, 2).reshape(LENGTH, WIDTH)
        gate_pre = jnp.dot(activated, w_glu, preferred_element_type=jnp.float32) + b_glu
        gated = activated.astype(jnp.float32) * jax.nn.sigmoid(gate_pre)
        scale = lax.rsqrt(lax.optimization_barrier(jnp.mean(gated * gated, axis=-1, keepdims=True)) + 1e-06)
        mixed = (gated * scale * g_mix).astype(jnp.bfloat16)
        return jnp.dot(mixed, w_out, preferred_element_type=jnp.float32).astype(jnp.bfloat16)
    return lax.map(per_sequence, jnp.arange(BATCH, dtype=jnp.int32))
```

```python
import functools
import math

import jax
import jax.numpy as jnp
from jax import lax
from jax.experimental import pallas as pl
from jax.experimental.pallas import tpu as pltpu
from jax.sharding import PartitionSpec as P

F32 = jnp.float32
BF16 = jnp.bfloat16
MESH = pl.DeviceIdType.MESH
LANES = 128
ORDERS = (("z", "y", "x"), ("y", "z", "x"), ("x", "z", "y"), ("z", "y", "x"), ("z", "x", "y"))
CUTS = len(ORDERS) - 1
SHARE = 0.28
VMEM_LIMIT = 56 * 1024 * 1024


def cmul(ar, ai, br, bi):
    return ar * br - ai * bi, ar * bi + ai * br


def powers(br, bi, count):
    row = lax.broadcasted_iota(jnp.int32, (8, br.shape[1]), 0)
    pr = jnp.ones((8, br.shape[1]), F32)
    pi = jnp.zeros((8, br.shape[1]), F32)
    sr, si = br, bi
    for bit in (1, 2, 4):
        qr, qi = cmul(pr, pi, sr, si)
        on = (row & bit) != 0
        pr, pi = jnp.where(on, qr, pr), jnp.where(on, qi, pi)
        sr, si = cmul(sr, si, sr, si)
    size = 8
    while size < count:
        qr, qi = cmul(pr, pi, sr, si)
        pr = jnp.concatenate([pr, qr], axis=0)
        pi = jnp.concatenate([pi, qi], axis=0)
        sr, si = cmul(sr, si, sr, si)
        size *= 2
    return pr, pi


def gelu(v):
    return 0.5 * v * (1.0 + jnp.tanh(math.sqrt(2.0 / math.pi) * (v + 0.044715 * (v * v * v))))


def kernel(
    dims, sizes,
    sig_hbm, a_real_hbm, a_imag_hbm, init_hbm, in_map_hbm, out_map_hbm, log_hbm, pace_hbm, skip_hbm, b_glu_hbm,
    g_mix_hbm, wg_hbm, wo_hbm, out,
    buf0, buf1, buf2, buf3, buf4, sig, a_real, a_imag, init, in_map, out_map, log_step, pace, skip, b_glu, g_mix,
    tx, rx, atx, arx, bars, cmat, inm,
    lsem, isem, wsend, wrecv, ssend, srecv, xsend, xrecv, asend, arecv,
):
    n_sp, n_dp, tokens, wd, fold, rows, states = sizes
    bufs = (buf0, buf1, buf2, buf3, buf4)
    pieces = range(len(ORDERS))
    me = lax.axis_index("sp")
    mx = lax.axis_index("dp")
    nx, nc, ny, nz = dims["x"], dims["c"], dims["y"], dims["z"]
    paired = n_dp == 2
    half = nx * ny * nz
    at = {"x": mx, "c": lax.rem(me, nc), "y": lax.rem(me // nc, ny), "z": me // (nc * ny)}
    ocols = wo_hbm.shape[1] // CUTS

    def device(where):
        return {"sp": (where["z"] * ny + where["y"]) * nc + where["c"], "dp": where["x"]}

    def index(where):
        return (where["x"] * ny + where["y"]) * nz + where["z"]

    def slot(t, where):
        return bufs[t].at[where["c"] * half + index(where)]

    loads = [
        pltpu.make_async_copy(src, dst, isem.at[j]) for j, (src, dst) in enumerate((
            (sig_hbm, sig), (a_real_hbm, a_real), (a_imag_hbm, a_imag), (init_hbm, init), (in_map_hbm, in_map),
            (out_map_hbm, out_map), (log_hbm, log_step), (pace_hbm, pace), (skip_hbm, skip), (b_glu_hbm, b_glu),
            (g_mix_hbm, g_mix)))
    ]
    local = [pltpu.make_async_copy(wg_hbm, slot(0, at), lsem.at[0])]
    for t in range(CUTS):
        local.append(pltpu.make_async_copy(
            wo_hbm.at[:, pl.ds(t * ocols, ocols)], slot(t + 1, at), lsem.at[t + 1]))
    for copy in loads[:1] + local + loads[1:]:
        copy.start()

    barrier = pltpu.get_barrier_semaphore()

    def greet(d, carry):
        pl.semaphore_signal(barrier, 1, device_id={"sp": lax.rem(me + d, n_sp), "dp": mx}, device_id_type=MESH)
        return carry

    def greet_all(d, carry):
        to = lax.rem(me * n_dp + mx + d, n_sp * n_dp)
        pl.semaphore_signal(barrier, 1, device_id={"sp": to // n_dp, "dp": lax.rem(to, n_dp)}, device_id_type=MESH)
        return carry

    if paired:
        lax.fori_loop(1, n_sp, greet, 0)
        pl.semaphore_signal(barrier, 1, device_id={"sp": me, "dp": 1 - mx}, device_id_type=MESH)
        greeted = n_sp
    else:
        lax.fori_loop(1, n_sp * n_dp, greet_all, 0)
        greeted = n_sp * n_dp - 1

    loads[0].wait()
    part = lax.broadcasted_iota(jnp.int32, (rows, LANES), 1) // wd
    for tile in range(sig.shape[1] // LANES):
        cut = [
            sig[p * rows:(p + 1) * rows, tile * LANES:(tile + 1) * LANES].astype(F32) for p in range(fold)
        ]
        for j in range(fold):
            acc = cut[j]
            for p in range(fold):
                if p != j:
                    moved = pltpu.roll(cut[p], ((p - j) * wd) % LANES, 1)
                    acc = jnp.where(part == p, moved, acc)
            tx[tile * fold + j] = acc.astype(BF16)

    pl.semaphore_wait(barrier, greeted)

    def chunk_copy(src, dst, ssem, rsem, to):
        return pltpu.make_async_remote_copy(
            src_ref=src, dst_ref=dst, send_sem=ssem, recv_sem=rsem,
            device_id={"sp": to, "dp": mx}, device_id_type=MESH)

    def send_chunk(d, carry):
        to = lax.rem(me + d, n_sp)
        chunk_copy(tx.at[to], rx.at[me], xsend.at[0], xrecv.at[me], to).start()
        return carry

    lax.fori_loop(1, n_sp, send_chunk, 0)

    def guarded(cond, action):
        if cond is None:
            action()
        else:
            pl.when(cond)(action)

    def hop(t, where, to):
        return pltpu.make_async_remote_copy(
            src_ref=slot(t, where), dst_ref=slot(t, where), send_sem=wsend.at[t],
            recv_sem=wrecv.at[t, index(where)], device_id=device(to), device_id_type=MESH)

    def across(t, ref):
        return pltpu.make_async_remote_copy(
            src_ref=ref, dst_ref=ref, send_sem=ssend.at[t], recv_sem=srecv.at[t],
            device_id=device(dict(at, c=1 - at["c"])), device_id_type=MESH)

    def source(move):
        where, cond = dict(at), None
        for axis, m in move.items():
            n, i = dims[axis], at[axis]
            if n == 2:
                where[axis] = 1 - i if m else i
            elif m:
                here = jnp.logical_and(i - m >= 0, i - m < n)
                cond = here if cond is None else jnp.logical_and(cond, here)
                where[axis] = jnp.clip(i - m, 0, n - 1)
        return where, cond

    def onward(order, move, level):
        found = []
        for deeper in range(level, len(order)):
            axis = order[deeper]
            n, m = dims[axis], move[axis]
            if n == 2:
                ways = () if m else (1,)
            else:
                ways = (1, -1) if m == 0 else ((m // abs(m),) if abs(m) < n - 1 else ())
            found += [(axis, way, deeper) for way in ways]
        return found

    def forward(t, move, level, first=False):
        where, cond = source(move)

        def act():
            if not first:
                hop(t, where, at).wait_recv()
            for axis, way, _ in onward(ORDERS[t], move, level):
                n, i = dims[axis], at[axis]
                if n == 2:
                    hop(t, where, dict(at, **{axis: 1 - i})).start()
                else:
                    ok = (i < n - 1) if way == 1 else (i > 0)
                    to = dict(at, **{axis: jnp.clip(i + way, 0, n - 1)})
                    pl.when(ok)(lambda to=to: hop(t, where, to).start())
            across(t, slot(t, where)).start()

        guarded(cond, act)

    def sends(t, z):
        total, wave = 0, [({axis: 0 for axis in ORDERS[t]}, 0)]
        while wave:
            later = []
            for move, level in wave:
                valid = 0 <= z - move["z"] < nz
                for axis, way, deeper in onward(ORDERS[t], move, level):
                    total += valid and (axis != "z" or 0 <= z + way < nz)
                    later.append((dict(move, **{axis: move[axis] + way}), deeper))
            wave = later
        return total

    def plan():
        waves, current = [], [(t, {axis: 0 for axis in ORDERS[t]}, 0) for t in pieces]
        while current:
            later = []
            for t, move, level in current:
                for axis, way, deeper in onward(ORDERS[t], move, level):
                    later.append((t, dict(move, **{axis: move[axis] + way}), deeper))
            waves += later
            current = later
        return waves

    def toss(t, d):
        to = lax.rem(me * n_dp + mx + d, n_sp * n_dp)
        return pltpu.make_async_remote_copy(
            src_ref=slot(t, at), dst_ref=slot(t, at), send_sem=wsend.at[t], recv_sem=wrecv.at[t, 0],
            device_id={"sp": to // n_dp, "dp": lax.rem(to, n_dp)}, device_id_type=MESH)

    for copy in local:
        copy.wait()
    events = []
    if paired:
        events = plan()
        for t in pieces:
            forward(t, {axis: 0 for axis in ORDERS[t]}, 0, True)
    else:
        for t in pieces:
            def toss_one(d, carry, t=t):
                toss(t, d).start()
                return carry

            lax.fori_loop(1, n_sp * n_dp, toss_one, 0)

    for copy in loads[1:]:
        copy.wait()
    groups, entries = a_real.shape
    channels = wd // groups
    lane_group = lax.broadcasted_iota(jnp.int32, (1, states), 1) // entries

    def row_of(ref, *lead):
        found = [ref[lead + (slice(g, g + 1), slice(None))] for g in range(groups)]
        return jnp.concatenate(found, axis=1)

    a_re, a_im = row_of(a_real), row_of(a_imag)
    logs = log_step[...]
    log_row = jnp.broadcast_to(logs[:, :1], (1, states))
    for g in range(1, groups):
        log_row = jnp.where(lane_group == g, jnp.broadcast_to(logs[:, g:g + 1], (1, states)), log_row)
    on = lax.broadcasted_iota(jnp.int32, (n_sp, n_sp), 0) == lax.broadcasted_iota(jnp.int32, (n_sp, n_sp), 1)
    paces = jnp.sum(jnp.where(on, jnp.broadcast_to(pace[...], (n_sp, n_sp)), 0.0), axis=1, keepdims=True)
    steps = paces * jnp.exp(log_row)

    def diagonal(blocks):
        lines = []
        for g in range(groups):
            line = [jnp.zeros((channels, entries), F32)] * groups
            line[g] = blocks[g]
            lines.append(jnp.concatenate(line, axis=1))
        return jnp.concatenate(lines, axis=0)

    for j in range(2):
        inm[j] = diagonal([in_map[g, j] for g in range(groups)])
    skips = jnp.concatenate([skip[...]] * fold, axis=1)
    real, angle = a_re * steps, a_im * steps
    decay, growth = jnp.exp(real), jnp.exp(-real)
    cos, sin = jnp.cos(angle), jnp.sin(angle)
    bar_re, bar_im = decay * cos, decay * sin
    modulus = a_re * a_re + a_im * a_im
    bars[0] = bar_re
    bars[1] = bar_im
    bars[2] = growth * cos
    bars[3] = -growth * sin
    bars[4] = ((bar_re - 1.0) * a_re + bar_im * a_im) / modulus
    bars[5] = (bar_im * a_re - (bar_re - 1.0) * a_im) / modulus
    for p in range(fold):
        for j in range(2):
            blank = [jnp.zeros((wd, states), BF16)] * fold
            blank[p] = diagonal([out_map[g, j] for g in range(groups)]).astype(BF16)
            cmat[2 * p + j] = jnp.concatenate(blank, axis=0)

    rx[me] = tx[me]

    span_row = lax.broadcasted_iota(jnp.int32, (tokens, tokens), 0)
    span_col = lax.broadcasted_iota(jnp.int32, (tokens, tokens), 1)
    tri = jnp.where(span_row >= span_col, 1.0, 0.0).astype(BF16)
    dot = functools.partial(jnp.dot, preferred_element_type=F32)

    def dot_t(a, b):
        return lax.dot_general(a, b, (((1,), (1,)), ((), ())), preferred_element_type=F32)

    inside = int(len(events) * SHARE)
    cuts = [inside * k // n_sp for k in range(n_sp + 1)]

    def block(k, carry):
        for i in range(n_sp):
            if cuts[i] < cuts[i + 1]:
                @pl.when(k == i)
                def _():
                    for event in events[cuts[i]:cuts[i + 1]]:
                        forward(*event)

        @pl.when(k != me)
        def _():
            chunk_copy(tx.at[me], rx.at[k], xsend.at[0], xrecv.at[k], me).wait_recv()

        before_re, before_im = carry
        br, bi, gr, gi, cr, ci = [bars[j, pl.ds(k, 1), :] for j in range(6)]
        chunk = rx[k]
        drive_re = (cr * inm[0] - ci * inm[1]).astype(BF16)
        drive_im = (cr * inm[1] + ci * inm[0]).astype(BF16)
        zero = jnp.zeros_like(drive_re)

        def inject(drive):
            return jnp.concatenate(
                [dot(chunk, jnp.concatenate([drive if q == p else zero for q in range(fold)], axis=0))
                 for p in range(fold)], axis=0)

        up_re, up_im = powers(gr, gi, tokens)
        sum_re, sum_im = cmul(inject(drive_re), inject(drive_im), up_re, up_im)
        sum_re, sum_im = dot(tri, sum_re.astype(BF16)), dot(tri, sum_im.astype(BF16))
        first_re, first_im = cmul(br, bi, before_re, before_im)
        down_re, down_im = powers(br, bi, tokens)
        state_re, state_im = cmul(sum_re + first_re, sum_im + first_im, down_re, down_im)
        s_re, s_im = state_re.astype(BF16), state_im.astype(BF16)
        response = skips * chunk.astype(F32)
        for p in range(fold):
            lines = slice(p * rows, (p + 1) * rows)
            response = response + dot_t(s_re[lines], cmat[2 * p]) - dot_t(s_im[lines], cmat[2 * p + 1])
        atx[k] = gelu(response).astype(BF16)

        @pl.when(k != me)
        def _():
            chunk_copy(atx.at[k], arx.at[me], asend.at[0], arecv.at[0], k).start()

        return state_re[tokens - 1:], state_im[tokens - 1:]

    lax.fori_loop(0, n_sp, block, (row_of(init, 0, 0), row_of(init, 0, 1)))

    arx[me] = atx[me]
    most = n_sp - 1
    chunk_copy(atx.at[pl.ds(0, most)], arx.at[pl.ds(0, most)], asend.at[0], arecv.at[0], me).wait_recv()
    tiles = []
    for tile in range(sig.shape[1] // LANES):
        chunks = [arx[tile * fold + j].astype(F32) for j in range(fold)]
        parts = []
        for p in range(fold):
            acc = chunks[p]
            for j in range(fold):
                if j != p:
                    moved = pltpu.roll(chunks[j], ((j - p) * wd) % LANES, 1)
                    acc = jnp.where(part == j, moved, acc)
            parts.append(acc)
        tiles.append(jnp.concatenate(parts, axis=0))
    act = jnp.concatenate(tiles, axis=1)
    act_bf = act.astype(BF16)

    def weight(t, x):
        found = []
        for i in range(n_sp):
            where = {"x": x, "c": i % nc, "z": i // (nc * ny), "y": (i // nc) % ny}
            found.append(bufs[t][where["c"] * half + index(where)])
        return jnp.concatenate(found, axis=0)

    rest = events[inside:]
    for event in rest:
        forward(*event)

    def complete(t):
        if paired:
            across(t, bufs[t].at[pl.ds((1 - at["c"]) * half, half)]).wait_recv()
        else:
            every = bufs[t].at[pl.ds(0, n_sp * n_dp - 1)]
            pltpu.make_async_remote_copy(
                src_ref=every, dst_ref=every, send_sem=wsend.at[t], recv_sem=wrecv.at[t, 0],
                device_id=device(at), device_id_type=MESH).wait_recv()

    complete(0)
    gate = jnp.concatenate([dot(act_bf, weight(0, x)) for x in range(n_dp)], axis=1)
    gated = act * jax.nn.sigmoid(gate + b_glu[...])
    scale = lax.rsqrt(jnp.mean(gated * gated, axis=-1, keepdims=True) + 1e-06)
    mixed = (gated * scale * g_mix[...]).astype(BF16)

    for t in range(1, CUTS + 1):
        complete(t)
        for x in range(n_dp):
            cols = slice((x * CUTS + t - 1) * ocols, (x * CUTS + t) * ocols)
            out[:, cols] = dot(mixed, weight(t, x)).astype(BF16)

    chunk_copy(tx.at[pl.ds(0, most)], rx.at[pl.ds(0, most)], xsend.at[0], xrecv.at[0], me).wait_send()
    chunk_copy(atx.at[pl.ds(0, most)], arx.at[pl.ds(0, most)], asend.at[0], arecv.at[0], me).wait_send()

    def drained(t, count):
        sent = bufs[t].at[pl.ds(0, count)]
        pltpu.make_async_remote_copy(
            src_ref=sent, dst_ref=sent, send_sem=wsend.at[t], recv_sem=wrecv.at[t, 0],
            device_id=device(at), device_id_type=MESH).wait_send()

    for t in pieces:
        if paired:
            across(t, bufs[t].at[pl.ds(at["c"] * half, half)]).wait_send()
            for z in range(nz):
                pl.when(at["z"] == z)(lambda z=z: drained(t, sends(t, z)))
        else:
            drained(t, n_sp * n_dp - 1)


def per_device(
    signal, pace, log_step, a_real, a_imag, in_map, out_map, skip, init_state, w_glu, b_glu, g_mix, w_out
):
    n_sp, n_dp = lax.axis_size("sp"), lax.axis_size("dp")
    tokens, width = signal.shape[1], signal.shape[2]
    groups, entries = a_real.shape
    channels = width // (groups * n_sp)
    wd = groups * channels
    states = groups * entries
    fold = LANES // wd
    rows = tokens // fold
    assert signal.shape[0] == 1 and pace.shape[1] == n_sp and n_sp % 4 == 0
    dims = {"x": n_dp, "c": 2, "y": 2, "z": n_sp // 4}
    wrows = w_out.shape[0]
    gcols, ocols = w_glu.shape[1], w_out.shape[1] // CUTS
    slots = n_sp * n_dp
    marks = slots // 2 if n_dp == 2 else 1
    chunk = pltpu.VMEM((n_sp, rows, LANES), BF16)
    sem = pltpu.SemaphoreType.DMA
    operands = (
        signal[0], a_real, a_imag, init_state, in_map.transpose(0, 1, 3, 2), out_map, log_step.reshape(1, -1), pace,
        skip.reshape(1, -1), b_glu.reshape(1, -1), g_mix.reshape(1, -1))
    output = pl.pallas_call(
        functools.partial(kernel, dims, (n_sp, n_dp, tokens, wd, fold, rows, states)),
        out_shape=pltpu.VMEM((tokens, w_out.shape[1] * n_dp), BF16),
        in_specs=[pl.BlockSpec(memory_space=pltpu.HBM)] * (len(operands) + 2),
        out_specs=pl.BlockSpec(memory_space=pltpu.VMEM),
        scratch_shapes=[
            pltpu.VMEM((slots, wrows, gcols if t == 0 else ocols), BF16) for t in range(len(ORDERS))
        ] + [pltpu.VMEM(x.shape, x.dtype) for x in operands] + [chunk] * 4 + [
            pltpu.VMEM((6, n_sp, states), F32),
            pltpu.VMEM((2 * fold, LANES, states), BF16),
            pltpu.VMEM((2, wd, states), F32),
            sem((len(ORDERS),)), sem((len(operands),)),
            sem((len(ORDERS),)), sem((len(ORDERS), marks)), sem((len(ORDERS),)), sem((len(ORDERS),)),
            sem((1,)), sem((n_sp,)), sem((1,)), sem((1,)),
        ],
        compiler_params=pltpu.CompilerParams(
            collective_id=0, has_side_effects=True, vmem_limit_bytes=VMEM_LIMIT),
    )(*operands, w_glu, w_out)
    return output[None]


def solution(mesh):
    in_specs = (
        P("dp", "sp", None),
        P("dp", None),
        P("sp"),
        P("sp", None),
        P("sp", None),
        P("sp", None, None, None),
        P("sp", None, None, None),
        P("sp"),
        P("dp", None, "sp", None),
        P("sp", "dp"),
        P(),
        P(),
        P("sp", "dp"),
    )
    out_specs = P("dp", "sp", None)
    return jax.shard_map(
        per_device, mesh=mesh, in_specs=in_specs, out_specs=out_specs, check_vma=False
    )
```

```python
import functools
import math

import jax
import jax.numpy as jnp
from jax import lax
from jax.experimental import pallas as pl
from jax.experimental.pallas import tpu as pltpu
from jax.sharding import PartitionSpec as P

F32 = jnp.float32
BF16 = jnp.bfloat16
MESH = pl.DeviceIdType.MESH
LANES = 128
ORDERS = (("z", "y", "x"), ("z", "y", "x"), ("x", "z", "y"), ("y", "z", "x"), ("z", "x", "y"))
CUTS = len(ORDERS) - 1
SHARE = 0.35
LAG = 0.2
AHEAD = 2
VMEM_LIMIT = 56 * 1024 * 1024


def cmul(ar, ai, br, bi):
    return ar * br - ai * bi, ar * bi + ai * br


def powers(br, bi, count):
    row = lax.broadcasted_iota(jnp.int32, (8, br.shape[1]), 0)
    pr = jnp.ones((8, br.shape[1]), F32)
    pi = jnp.zeros((8, br.shape[1]), F32)
    sr, si = br, bi
    for bit in (1, 2, 4):
        qr, qi = cmul(pr, pi, sr, si)
        on = (row & bit) != 0
        pr, pi = jnp.where(on, qr, pr), jnp.where(on, qi, pi)
        sr, si = cmul(sr, si, sr, si)
    size = 8
    while size < count:
        qr, qi = cmul(pr, pi, sr, si)
        pr = jnp.concatenate([pr, qr], axis=0)
        pi = jnp.concatenate([pi, qi], axis=0)
        sr, si = cmul(sr, si, sr, si)
        size *= 2
    return pr, pi


def gelu(v):
    return 0.5 * v * (1.0 + jnp.tanh(math.sqrt(2.0 / math.pi) * (v + 0.044715 * (v * v * v))))


def kernel(
    dims, sizes,
    sig_hbm, a_real_hbm, a_imag_hbm, init_hbm, in_map_hbm, out_map_hbm, log_hbm, pace_hbm, skip_hbm, b_glu_hbm,
    g_mix_hbm, wg_hbm, wo_hbm, out,
    buf0, buf1, buf2, buf3, buf4, sig, a_real, a_imag, init, in_map, out_map, log_step, pace, skip, b_glu, g_mix,
    tx, rx, atx, arx, bars, cmat, inm,
    lsem, isem, wsend, wrecv, ssend, srecv, xsend, xrecv, asend, arecv,
):
    n_sp, n_dp, tokens, wd, fold, rows, states = sizes
    bufs = (buf0, buf1, buf2, buf3, buf4)
    pieces = range(len(ORDERS))
    me = lax.axis_index("sp")
    mx = lax.axis_index("dp")
    nx, nc, ny, nz = dims["x"], dims["c"], dims["y"], dims["z"]
    paired = n_dp == 2
    half = nx * ny * nz
    at = {"x": mx, "c": lax.rem(me, nc), "y": lax.rem(me // nc, ny), "z": me // (nc * ny)}
    ocols = wo_hbm.shape[1] // CUTS

    def device(where):
        return {"sp": (where["z"] * ny + where["y"]) * nc + where["c"], "dp": where["x"]}

    def index(where):
        return (where["x"] * ny + where["y"]) * nz + where["z"]

    def slot(t, where):
        return bufs[t].at[where["c"] * half + index(where)]

    loads = [
        pltpu.make_async_copy(src, dst, isem.at[j]) for j, (src, dst) in enumerate((
            (sig_hbm, sig), (a_real_hbm, a_real), (a_imag_hbm, a_imag), (init_hbm, init), (in_map_hbm, in_map),
            (out_map_hbm, out_map), (log_hbm, log_step), (pace_hbm, pace), (skip_hbm, skip), (b_glu_hbm, b_glu),
            (g_mix_hbm, g_mix)))
    ]
    local = [pltpu.make_async_copy(wg_hbm, slot(0, at), lsem.at[0])]
    for t in range(CUTS):
        local.append(pltpu.make_async_copy(
            wo_hbm.at[:, pl.ds(t * ocols, ocols)], slot(t + 1, at), lsem.at[t + 1]))

    barrier = pltpu.get_barrier_semaphore()

    def greet(d, carry):
        pl.semaphore_signal(barrier, 1, device_id={"sp": lax.rem(me + d, n_sp), "dp": mx}, device_id_type=MESH)
        return carry

    def greet_all(d, carry):
        to = lax.rem(me * n_dp + mx + d, n_sp * n_dp)
        pl.semaphore_signal(barrier, 1, device_id={"sp": to // n_dp, "dp": lax.rem(to, n_dp)}, device_id_type=MESH)
        return carry

    if paired:
        lax.fori_loop(1, n_sp, greet, 0)
        pl.semaphore_signal(barrier, 1, device_id={"sp": me, "dp": 1 - mx}, device_id_type=MESH)
        greeted = n_sp
    else:
        lax.fori_loop(1, n_sp * n_dp, greet_all, 0)
        greeted = n_sp * n_dp - 1

    for copy in loads[:1] + local + loads[1:]:
        copy.start()
    loads[0].wait()
    part = lax.broadcasted_iota(jnp.int32, (rows, LANES), 1) // wd
    for tile in range(sig.shape[1] // LANES):
        cut = [
            sig[p * rows:(p + 1) * rows, tile * LANES:(tile + 1) * LANES].astype(F32) for p in range(fold)
        ]
        for j in range(fold):
            acc = cut[j]
            for p in range(fold):
                if p != j:
                    moved = pltpu.roll(cut[p], ((p - j) * wd) % LANES, 1)
                    acc = jnp.where(part == p, moved, acc)
            tx[tile * fold + j] = acc.astype(BF16)

    pl.semaphore_wait(barrier, greeted)

    def chunk_copy(src, dst, ssem, rsem, to):
        return pltpu.make_async_remote_copy(
            src_ref=src, dst_ref=dst, send_sem=ssem, recv_sem=rsem,
            device_id={"sp": to, "dp": mx}, device_id_type=MESH)

    def send_chunk(d, carry):
        to = lax.rem(me + d, n_sp)
        chunk_copy(tx.at[to], rx.at[me], xsend.at[0], xrecv.at[me], to).start()
        return carry

    lax.fori_loop(1, n_sp, send_chunk, 0)

    def guarded(cond, action):
        if cond is None:
            action()
        else:
            pl.when(cond)(action)

    def hop(t, where, to):
        return pltpu.make_async_remote_copy(
            src_ref=slot(t, where), dst_ref=slot(t, where), send_sem=wsend.at[t],
            recv_sem=wrecv.at[t, index(where)], device_id=device(to), device_id_type=MESH)

    def across(t, ref):
        return pltpu.make_async_remote_copy(
            src_ref=ref, dst_ref=ref, send_sem=ssend.at[t], recv_sem=srecv.at[t],
            device_id=device(dict(at, c=1 - at["c"])), device_id_type=MESH)

    def source(move):
        where, cond = dict(at), None
        for axis, m in move.items():
            n, i = dims[axis], at[axis]
            if n == 2:
                where[axis] = 1 - i if m else i
            elif m:
                here = jnp.logical_and(i - m >= 0, i - m < n)
                cond = here if cond is None else jnp.logical_and(cond, here)
                where[axis] = jnp.clip(i - m, 0, n - 1)
        return where, cond

    def onward(order, move, level):
        found = []
        for deeper in range(level, len(order)):
            axis = order[deeper]
            n, m = dims[axis], move[axis]
            if n == 2:
                ways = () if m else (1,)
            else:
                ways = (1, -1) if m == 0 else ((m // abs(m),) if abs(m) < n - 1 else ())
            found += [(axis, way, deeper) for way in ways]
        return found

    def forward(t, move, level, first=False):
        where, cond = source(move)

        def act():
            if not first:
                hop(t, where, at).wait_recv()
            for axis, way, _ in onward(ORDERS[t], move, level):
                n, i = dims[axis], at[axis]
                if n == 2:
                    hop(t, where, dict(at, **{axis: 1 - i})).start()
                else:
                    ok = (i < n - 1) if way == 1 else (i > 0)
                    to = dict(at, **{axis: jnp.clip(i + way, 0, n - 1)})
                    pl.when(ok)(lambda to=to: hop(t, where, to).start())
            across(t, slot(t, where)).start()

        guarded(cond, act)

    def sends(t, z):
        total, wave = 0, [({axis: 0 for axis in ORDERS[t]}, 0)]
        while wave:
            later = []
            for move, level in wave:
                valid = 0 <= z - move["z"] < nz
                for axis, way, deeper in onward(ORDERS[t], move, level):
                    total += valid and (axis != "z" or 0 <= z + way < nz)
                    later.append((dict(move, **{axis: move[axis] + way}), deeper))
            wave = later
        return total

    def plan():
        waves, current = [], [(t, {axis: 0 for axis in ORDERS[t]}, 0) for t in pieces]
        depth = 0
        while current:
            later = []
            for t, move, level in current:
                for axis, way, deeper in onward(ORDERS[t], move, level):
                    later.append((t, dict(move, **{axis: move[axis] + way}), deeper))
            waves += [(depth + LAG * event[0], event) for event in later]
            current, depth = later, depth + 1
        return [event for _, event in sorted(waves, key=lambda found: found[0])]

    def toss(t, d):
        to = lax.rem(me * n_dp + mx + d, n_sp * n_dp)
        return pltpu.make_async_remote_copy(
            src_ref=slot(t, at), dst_ref=slot(t, at), send_sem=wsend.at[t], recv_sem=wrecv.at[t, 0],
            device_id={"sp": to // n_dp, "dp": lax.rem(to, n_dp)}, device_id_type=MESH)

    for copy in local:
        copy.wait()
    events = []
    if paired:
        events = plan()
        for t in pieces:
            forward(t, {axis: 0 for axis in ORDERS[t]}, 0, True)
    else:
        for t in pieces:
            def toss_one(d, carry, t=t):
                toss(t, d).start()
                return carry

            lax.fori_loop(1, n_sp * n_dp, toss_one, 0)

    for copy in loads[1:]:
        copy.wait()
    groups, entries = a_real.shape
    channels = wd // groups
    lane_group = lax.broadcasted_iota(jnp.int32, (1, states), 1) // entries

    def row_of(ref, *lead):
        found = [ref[lead + (slice(g, g + 1), slice(None))] for g in range(groups)]
        return jnp.concatenate(found, axis=1)

    a_re, a_im = row_of(a_real), row_of(a_imag)
    logs = log_step[...]
    log_row = jnp.broadcast_to(logs[:, :1], (1, states))
    for g in range(1, groups):
        log_row = jnp.where(lane_group == g, jnp.broadcast_to(logs[:, g:g + 1], (1, states)), log_row)
    on = lax.broadcasted_iota(jnp.int32, (n_sp, n_sp), 0) == lax.broadcasted_iota(jnp.int32, (n_sp, n_sp), 1)
    paces = jnp.sum(jnp.where(on, jnp.broadcast_to(pace[...], (n_sp, n_sp)), 0.0), axis=1, keepdims=True)
    steps = paces * jnp.exp(log_row)

    def diagonal(blocks):
        lines = []
        for g in range(groups):
            line = [jnp.zeros((channels, entries), F32)] * groups
            line[g] = blocks[g]
            lines.append(jnp.concatenate(line, axis=1))
        return jnp.concatenate(lines, axis=0)

    for j in range(2):
        inm[j] = diagonal([in_map[g, j] for g in range(groups)])
    skips = jnp.concatenate([skip[...]] * fold, axis=1)
    real, angle = a_re * steps, a_im * steps
    decay, growth = jnp.exp(real), jnp.exp(-real)
    cos, sin = jnp.cos(angle), jnp.sin(angle)
    bar_re, bar_im = decay * cos, decay * sin
    modulus = a_re * a_re + a_im * a_im
    bars[0] = bar_re
    bars[1] = bar_im
    bars[2] = growth * cos
    bars[3] = -growth * sin
    bars[4] = ((bar_re - 1.0) * a_re + bar_im * a_im) / modulus
    bars[5] = (bar_im * a_re - (bar_re - 1.0) * a_im) / modulus
    for p in range(fold):
        for j in range(2):
            blank = [jnp.zeros((wd, states), BF16)] * fold
            blank[p] = diagonal([out_map[g, j] for g in range(groups)]).astype(BF16)
            cmat[2 * p + j] = jnp.concatenate(blank, axis=0)

    rx[me] = tx[me]

    span_row = lax.broadcasted_iota(jnp.int32, (tokens, tokens), 0)
    span_col = lax.broadcasted_iota(jnp.int32, (tokens, tokens), 1)
    tri = jnp.where(span_row >= span_col, 1.0, 0.0).astype(BF16)
    dot = functools.partial(jnp.dot, preferred_element_type=F32)

    def dot_t(a, b):
        return lax.dot_general(a, b, (((1,), (1,)), ((), ())), preferred_element_type=F32)

    inside = int(len(events) * SHARE)
    cuts = [inside * k // n_sp for k in range(n_sp + 1)]

    def block(k, carry):
        for i in range(n_sp):
            if cuts[i] < cuts[i + 1]:
                @pl.when(k == i)
                def _():
                    for event in events[cuts[i]:cuts[i + 1]]:
                        forward(*event)

        @pl.when(k != me)
        def _():
            chunk_copy(tx.at[me], rx.at[k], xsend.at[0], xrecv.at[k], me).wait_recv()

        before_re, before_im = carry
        br, bi, gr, gi, cr, ci = [bars[j, pl.ds(k, 1), :] for j in range(6)]
        chunk = rx[k]
        drive_re = (cr * inm[0] - ci * inm[1]).astype(BF16)
        drive_im = (cr * inm[1] + ci * inm[0]).astype(BF16)
        zero = jnp.zeros_like(drive_re)

        def inject(drive):
            return jnp.concatenate(
                [dot(chunk, jnp.concatenate([drive if q == p else zero for q in range(fold)], axis=0))
                 for p in range(fold)], axis=0)

        up_re, up_im = powers(gr, gi, tokens)
        sum_re, sum_im = cmul(inject(drive_re), inject(drive_im), up_re, up_im)
        sum_re, sum_im = dot(tri, sum_re.astype(BF16)), dot(tri, sum_im.astype(BF16))
        first_re, first_im = cmul(br, bi, before_re, before_im)
        down_re, down_im = powers(br, bi, tokens)
        state_re, state_im = cmul(sum_re + first_re, sum_im + first_im, down_re, down_im)
        s_re, s_im = state_re.astype(BF16), state_im.astype(BF16)
        response = skips * chunk.astype(F32)
        for p in range(fold):
            lines = slice(p * rows, (p + 1) * rows)
            response = response + dot_t(s_re[lines], cmat[2 * p]) - dot_t(s_im[lines], cmat[2 * p + 1])
        atx[k] = gelu(response).astype(BF16)

        @pl.when(k != me)
        def _():
            chunk_copy(atx.at[k], arx.at[me], asend.at[0], arecv.at[0], k).start()

        return state_re[tokens - 1:], state_im[tokens - 1:]

    lax.fori_loop(0, n_sp, block, (row_of(init, 0, 0), row_of(init, 0, 1)))

    most = n_sp - 1

    def weight(t, x):
        found = []
        for i in range(n_sp):
            where = {"x": x, "c": i % nc, "z": i // (nc * ny), "y": (i // nc) % ny}
            found.append(bufs[t][where["c"] * half + index(where)])
        return jnp.concatenate(found, axis=0)

    def complete(t):
        if paired:
            across(t, bufs[t].at[pl.ds((1 - at["c"]) * half, half)]).wait_recv()
        else:
            every = bufs[t].at[pl.ds(0, n_sp * n_dp - 1)]
            pltpu.make_async_remote_copy(
                src_ref=every, dst_ref=every, send_sem=wsend.at[t], recv_sem=wrecv.at[t, 0],
                device_id=device(at), device_id_type=MESH).wait_recv()

    def activated():
        arx[me] = atx[me]
        chunk_copy(atx.at[pl.ds(0, most)], arx.at[pl.ds(0, most)], asend.at[0], arecv.at[0], me).wait_recv()
        tiles = []
        for tile in range(sig.shape[1] // LANES):
            chunks = [arx[tile * fold + j].astype(F32) for j in range(fold)]
            parts = []
            for p in range(fold):
                acc = chunks[p]
                for j in range(fold):
                    if j != p:
                        moved = pltpu.roll(chunks[j], ((j - p) * wd) % LANES, 1)
                        acc = jnp.where(part == j, moved, acc)
                parts.append(acc)
            tiles.append(jnp.concatenate(parts, axis=0))
        return jnp.concatenate(tiles, axis=1)

    rest = events[inside:]
    mixed = None
    for t in pieces:
        soon = t if t == 0 else t + AHEAD
        last = max((i for i, event in enumerate(rest) if event[0] <= soon), default=-1)
        for event in rest[:last + 1]:
            forward(*event)
        rest = rest[last + 1:]
        if t == 0:
            act = activated()
            complete(0)
            gate = jnp.concatenate([dot(act.astype(BF16), weight(0, x)) for x in range(n_dp)], axis=1)
            gated = act * jax.nn.sigmoid(gate + b_glu[...])
            scale = lax.rsqrt(jnp.mean(gated * gated, axis=-1, keepdims=True) + 1e-06)
            mixed = (gated * scale * g_mix[...]).astype(BF16)
        else:
            complete(t)
            for x in range(n_dp):
                cols = slice((x * CUTS + t - 1) * ocols, (x * CUTS + t) * ocols)
                out[:, cols] = dot(mixed, weight(t, x)).astype(BF16)

    chunk_copy(tx.at[pl.ds(0, most)], rx.at[pl.ds(0, most)], xsend.at[0], xrecv.at[0], me).wait_send()
    chunk_copy(atx.at[pl.ds(0, most)], arx.at[pl.ds(0, most)], asend.at[0], arecv.at[0], me).wait_send()

    def drained(t, count):
        sent = bufs[t].at[pl.ds(0, count)]
        pltpu.make_async_remote_copy(
            src_ref=sent, dst_ref=sent, send_sem=wsend.at[t], recv_sem=wrecv.at[t, 0],
            device_id=device(at), device_id_type=MESH).wait_send()

    for t in pieces:
        if paired:
            across(t, bufs[t].at[pl.ds(at["c"] * half, half)]).wait_send()
            for z in range(nz):
                pl.when(at["z"] == z)(lambda z=z: drained(t, sends(t, z)))
        else:
            drained(t, n_sp * n_dp - 1)


def per_device(
    signal, pace, log_step, a_real, a_imag, in_map, out_map, skip, init_state, w_glu, b_glu, g_mix, w_out
):
    n_sp, n_dp = lax.axis_size("sp"), lax.axis_size("dp")
    tokens, width = signal.shape[1], signal.shape[2]
    groups, entries = a_real.shape
    channels = width // (groups * n_sp)
    wd = groups * channels
    states = groups * entries
    fold = LANES // wd
    rows = tokens // fold
    assert signal.shape[0] == 1 and pace.shape[1] == n_sp and n_sp % 4 == 0
    dims = {"x": n_dp, "c": 2, "y": 2, "z": n_sp // 4}
    wrows = w_out.shape[0]
    gcols, ocols = w_glu.shape[1], w_out.shape[1] // CUTS
    slots = n_sp * n_dp
    marks = slots // 2 if n_dp == 2 else 1
    chunk = pltpu.VMEM((n_sp, rows, LANES), BF16)
    sem = pltpu.SemaphoreType.DMA
    operands = (
        signal[0], a_real, a_imag, init_state, in_map.transpose(0, 1, 3, 2), out_map, log_step.reshape(1, -1), pace,
        skip.reshape(1, -1), b_glu.reshape(1, -1), g_mix.reshape(1, -1))
    output = pl.pallas_call(
        functools.partial(kernel, dims, (n_sp, n_dp, tokens, wd, fold, rows, states)),
        out_shape=pltpu.VMEM((tokens, w_out.shape[1] * n_dp), BF16),
        in_specs=[pl.BlockSpec(memory_space=pltpu.HBM)] * (len(operands) + 2),
        out_specs=pl.BlockSpec(memory_space=pltpu.VMEM),
        scratch_shapes=[
            pltpu.VMEM((slots, wrows, gcols if t == 0 else ocols), BF16) for t in range(len(ORDERS))
        ] + [pltpu.VMEM(x.shape, x.dtype) for x in operands] + [chunk] * 4 + [
            pltpu.VMEM((6, n_sp, states), F32),
            pltpu.VMEM((2 * fold, LANES, states), BF16),
            pltpu.VMEM((2, wd, states), F32),
            sem((len(ORDERS),)), sem((len(operands),)),
            sem((len(ORDERS),)), sem((len(ORDERS), marks)), sem((len(ORDERS),)), sem((len(ORDERS),)),
            sem((1,)), sem((n_sp,)), sem((1,)), sem((1,)),
        ],
        compiler_params=pltpu.CompilerParams(
            collective_id=0, has_side_effects=True, vmem_limit_bytes=VMEM_LIMIT),
    )(*operands, w_glu, w_out)
    return output[None]


def solution(mesh):
    in_specs = (
        P("dp", "sp", None),
        P("dp", None),
        P("sp"),
        P("sp", None),
        P("sp", None),
        P("sp", None, None, None),
        P("sp", None, None, None),
        P("sp"),
        P("dp", None, "sp", None),
        P("sp", "dp"),
        P(),
        P(),
        P("sp", "dp"),
    )
    out_specs = P("dp", "sp", None)
    return jax.shard_map(
        per_device, mesh=mesh, in_specs=in_specs, out_specs=out_specs, check_vma=False
    )
```

```python
import functools
import math

import jax
import jax.numpy as jnp
from jax import lax
from jax.experimental import pallas as pl
from jax.experimental.pallas import tpu as pltpu
from jax.sharding import PartitionSpec as P

F32 = jnp.float32
BF16 = jnp.bfloat16
MESH = pl.DeviceIdType.MESH
LANES = 128
ORDERS = (("z", "y", "x"), ("z", "y", "x"), ("x", "z", "y"), ("y", "z", "x"), ("z", "x", "y"))
CUTS = len(ORDERS) - 1
SHARE = 0.5
PRE = 0.14
LAGS = (0.0, 0.2, 0.4, 0.6, 0.8)
AHEAD = 3
VMEM_LIMIT = 56 * 1024 * 1024


def cmul(ar, ai, br, bi):
    return ar * br - ai * bi, ar * bi + ai * br


def powers(br, bi, count):
    row = lax.broadcasted_iota(jnp.int32, (8, br.shape[1]), 0)
    pr = jnp.ones((8, br.shape[1]), F32)
    pi = jnp.zeros((8, br.shape[1]), F32)
    sr, si = br, bi
    for bit in (1, 2, 4):
        qr, qi = cmul(pr, pi, sr, si)
        on = (row & bit) != 0
        pr, pi = jnp.where(on, qr, pr), jnp.where(on, qi, pi)
        sr, si = cmul(sr, si, sr, si)
    size = 8
    while size < count:
        qr, qi = cmul(pr, pi, sr, si)
        pr = jnp.concatenate([pr, qr], axis=0)
        pi = jnp.concatenate([pi, qi], axis=0)
        sr, si = cmul(sr, si, sr, si)
        size *= 2
    return pr, pi


def gelu(v):
    return 0.5 * v * (1.0 + jnp.tanh(math.sqrt(2.0 / math.pi) * (v + 0.044715 * (v * v * v))))


def kernel(
    dims, sizes,
    sig_hbm, a_real_hbm, a_imag_hbm, init_hbm, in_map_hbm, out_map_hbm, log_hbm, pace_hbm, skip_hbm, b_glu_hbm,
    g_mix_hbm, wg_hbm, wo_hbm, out,
    buf0, buf1, buf2, buf3, buf4, sig, a_real, a_imag, init, in_map, out_map, log_step, pace, skip, b_glu, g_mix,
    tx, rx, atx, arx, bars, cmat, inm,
    ready, lsem, isem, wsend, wrecv, ssend, srecv, xsend, xrecv, asend, arecv,
):
    n_sp, n_dp, tokens, wd, fold, rows, states = sizes
    bufs = (buf0, buf1, buf2, buf3, buf4)
    pieces = range(len(ORDERS))
    me = lax.axis_index("sp")
    mx = lax.axis_index("dp")
    nx, nc, ny, nz = dims["x"], dims["c"], dims["y"], dims["z"]
    paired = n_dp == 2
    half = nx * ny * nz
    at = {"x": mx, "c": lax.rem(me, nc), "y": lax.rem(me // nc, ny), "z": me // (nc * ny)}
    ocols = wo_hbm.shape[1] // CUTS

    def device(where):
        return {"sp": (where["z"] * ny + where["y"]) * nc + where["c"], "dp": where["x"]}

    def index(where):
        return (where["x"] * ny + where["y"]) * nz + where["z"]

    def slot(t, where):
        return bufs[t].at[where["c"] * half + index(where)]

    loads = [
        pltpu.make_async_copy(src, dst, isem.at[j]) for j, (src, dst) in enumerate((
            (sig_hbm, sig), (a_real_hbm, a_real), (a_imag_hbm, a_imag), (init_hbm, init), (in_map_hbm, in_map),
            (out_map_hbm, out_map), (log_hbm, log_step), (pace_hbm, pace), (skip_hbm, skip), (b_glu_hbm, b_glu),
            (g_mix_hbm, g_mix)))
    ]
    local = [pltpu.make_async_copy(wg_hbm, slot(0, at), lsem.at[0])]
    for t in range(CUTS):
        local.append(pltpu.make_async_copy(
            wo_hbm.at[:, pl.ds(t * ocols, ocols)], slot(t + 1, at), lsem.at[t + 1]))

    barrier = pltpu.get_barrier_semaphore()

    def guarded(cond, action):
        if cond is None:
            action()
        else:
            pl.when(cond)(action)

    def step(axis, way):
        n, i = dims[axis], at[axis]
        if n == 2:
            return dict(at, **{axis: 1 - i}), None
        return dict(at, **{axis: jnp.clip(i + way, 0, n - 1)}), (i < n - 1) if way == 1 else (i > 0)

    ways = [(axis, way) for axis in ("z", "y", "x", "c") for way in ((1,) if dims[axis] == 2 else (1, -1))]

    def tell(semaphore, axis, way):
        to, ok = step(axis, way)
        guarded(ok, lambda: pl.semaphore_signal(semaphore, 1, device_id=device(to), device_id_type=MESH))

    def hear(semaphore, axis, way):
        guarded(step(axis, way)[1], lambda: pl.semaphore_wait(semaphore, 1))

    def greet_all(d, carry):
        to = lax.rem(me * n_dp + mx + d, n_sp * n_dp)
        pl.semaphore_signal(barrier, 1, device_id={"sp": to // n_dp, "dp": lax.rem(to, n_dp)}, device_id_type=MESH)
        return carry

    if paired:
        for axis, way in ways:
            tell(barrier, axis, way)
    else:
        lax.fori_loop(1, n_sp * n_dp, greet_all, 0)

    for copy in loads[:1] + local + loads[1:]:
        copy.start()
    if paired:
        peers = [step(axis, way)[1] for axis, way in ways]
        pl.semaphore_wait(barrier, sum(1 if ok is None else jnp.where(ok, 1, 0) for ok in peers))
    else:
        pl.semaphore_wait(barrier, n_sp * n_dp - 1)

    def hop(t, where, to):
        return pltpu.make_async_remote_copy(
            src_ref=slot(t, where), dst_ref=slot(t, where), send_sem=wsend.at[t],
            recv_sem=wrecv.at[t, index(where)], device_id=device(to), device_id_type=MESH)

    def across(t, ref):
        return pltpu.make_async_remote_copy(
            src_ref=ref, dst_ref=ref, send_sem=ssend.at[t], recv_sem=srecv.at[t],
            device_id=device(dict(at, c=1 - at["c"])), device_id_type=MESH)

    def source(move):
        where, cond = dict(at), None
        for axis, m in move.items():
            n, i = dims[axis], at[axis]
            if n == 2:
                where[axis] = 1 - i if m else i
            elif m:
                here = jnp.logical_and(i - m >= 0, i - m < n)
                cond = here if cond is None else jnp.logical_and(cond, here)
                where[axis] = jnp.clip(i - m, 0, n - 1)
        return where, cond

    def onward(order, move, level):
        found = []
        for deeper in range(level, len(order)):
            axis = order[deeper]
            n, m = dims[axis], move[axis]
            if n == 2:
                ways = () if m else (1,)
            else:
                ways = (1, -1) if m == 0 else ((m // abs(m),) if abs(m) < n - 1 else ())
            found += [(axis, way, deeper) for way in ways]
        return found

    def forward(t, move, level, first=False):
        where, cond = source(move)

        def act():
            if not first:
                hop(t, where, at).wait_recv()
            for axis, way, _ in onward(ORDERS[t], move, level):
                n, i = dims[axis], at[axis]
                if n == 2:
                    hop(t, where, dict(at, **{axis: 1 - i})).start()
                else:
                    ok = (i < n - 1) if way == 1 else (i > 0)
                    to = dict(at, **{axis: jnp.clip(i + way, 0, n - 1)})
                    pl.when(ok)(lambda to=to: hop(t, where, to).start())
            across(t, slot(t, where)).start()

        guarded(cond, act)

    def sends(t, z):
        total, wave = 0, [({axis: 0 for axis in ORDERS[t]}, 0)]
        while wave:
            later = []
            for move, level in wave:
                valid = 0 <= z - move["z"] < nz
                for axis, way, deeper in onward(ORDERS[t], move, level):
                    total += valid and (axis != "z" or 0 <= z + way < nz)
                    later.append((dict(move, **{axis: move[axis] + way}), deeper))
            wave = later
        return total

    def plan():
        waves, current = [], [(t, {axis: 0 for axis in ORDERS[t]}, 0) for t in pieces]
        depth = 0
        while current:
            later = []
            for t, move, level in current:
                for axis, way, deeper in onward(ORDERS[t], move, level):
                    later.append((t, dict(move, **{axis: move[axis] + way}), deeper))
            waves += [(depth + LAGS[event[0]], event) for event in later]
            current, depth = later, depth + 1
        return [event for _, event in sorted(waves, key=lambda found: found[0])]

    def toss(t, d):
        to = lax.rem(me * n_dp + mx + d, n_sp * n_dp)
        return pltpu.make_async_remote_copy(
            src_ref=slot(t, at), dst_ref=slot(t, at), send_sem=wsend.at[t], recv_sem=wrecv.at[t, 0],
            device_id={"sp": to // n_dp, "dp": lax.rem(to, n_dp)}, device_id_type=MESH)

    for copy in local:
        copy.wait()
    events = []
    if paired:
        events = plan()
        for t in pieces:
            forward(t, {axis: 0 for axis in ORDERS[t]}, 0, True)
    else:
        for t in pieces:
            def toss_one(d, carry, t=t):
                toss(t, d).start()
                return carry

            lax.fori_loop(1, n_sp * n_dp, toss_one, 0)

    loads[0].wait()
    part = lax.broadcasted_iota(jnp.int32, (rows, LANES), 1) // wd
    for tile in range(sig.shape[1] // LANES):
        cut = [
            sig[p * rows:(p + 1) * rows, tile * LANES:(tile + 1) * LANES].astype(F32) for p in range(fold)
        ]
        for j in range(fold):
            acc = cut[j]
            for p in range(fold):
                if p != j:
                    moved = pltpu.roll(cut[p], ((p - j) * wd) % LANES, 1)
                    acc = jnp.where(part == p, moved, acc)
            tx[tile * fold + j] = acc.astype(BF16)

    if paired:
        if dims["z"] > 2:
            for way in (1, -1):
                hear(ready.at[0 if way == 1 else 1], "z", -way)
                tell(ready.at[0 if way == 1 else 1], "z", way)
        else:
            tell(ready.at[0], "z", 1)
            hear(ready.at[0], "z", 1)
        for j, axis in ((2, "y"), (3, "c")):
            tell(ready.at[j], axis, 1)
            hear(ready.at[j], axis, 1)

    def chunk_copy(src, dst, ssem, rsem, to):
        return pltpu.make_async_remote_copy(
            src_ref=src, dst_ref=dst, send_sem=ssem, recv_sem=rsem,
            device_id={"sp": to, "dp": mx}, device_id_type=MESH)

    def send_chunk(d, carry):
        to = lax.rem(me + d, n_sp)
        chunk_copy(tx.at[to], rx.at[me], xsend.at[0], xrecv.at[me], to).start()
        return carry

    lax.fori_loop(1, n_sp, send_chunk, 0)

    for copy in loads[1:]:
        copy.wait()
    groups, entries = a_real.shape
    channels = wd // groups
    lane_group = lax.broadcasted_iota(jnp.int32, (1, states), 1) // entries

    def row_of(ref, *lead):
        found = [ref[lead + (slice(g, g + 1), slice(None))] for g in range(groups)]
        return jnp.concatenate(found, axis=1)

    a_re, a_im = row_of(a_real), row_of(a_imag)
    logs = log_step[...]
    log_row = jnp.broadcast_to(logs[:, :1], (1, states))
    for g in range(1, groups):
        log_row = jnp.where(lane_group == g, jnp.broadcast_to(logs[:, g:g + 1], (1, states)), log_row)
    on = lax.broadcasted_iota(jnp.int32, (n_sp, n_sp), 0) == lax.broadcasted_iota(jnp.int32, (n_sp, n_sp), 1)
    paces = jnp.sum(jnp.where(on, jnp.broadcast_to(pace[...], (n_sp, n_sp)), 0.0), axis=1, keepdims=True)
    steps = paces * jnp.exp(log_row)

    def diagonal(blocks):
        lines = []
        for g in range(groups):
            line = [jnp.zeros((channels, entries), F32)] * groups
            line[g] = blocks[g]
            lines.append(jnp.concatenate(line, axis=1))
        return jnp.concatenate(lines, axis=0)

    for j in range(2):
        inm[j] = diagonal([in_map[g, j] for g in range(groups)])
    skips = jnp.concatenate([skip[...]] * fold, axis=1)
    real, angle = a_re * steps, a_im * steps
    decay, growth = jnp.exp(real), jnp.exp(-real)
    cos, sin = jnp.cos(angle), jnp.sin(angle)
    bar_re, bar_im = decay * cos, decay * sin
    modulus = a_re * a_re + a_im * a_im
    bars[0] = bar_re
    bars[1] = bar_im
    bars[2] = growth * cos
    bars[3] = -growth * sin
    bars[4] = ((bar_re - 1.0) * a_re + bar_im * a_im) / modulus
    bars[5] = (bar_im * a_re - (bar_re - 1.0) * a_im) / modulus
    for p in range(fold):
        for j in range(2):
            blank = [jnp.zeros((wd, states), BF16)] * fold
            blank[p] = diagonal([out_map[g, j] for g in range(groups)]).astype(BF16)
            cmat[2 * p + j] = jnp.concatenate(blank, axis=0)

    rx[me] = tx[me]

    span_row = lax.broadcasted_iota(jnp.int32, (tokens, tokens), 0)
    span_col = lax.broadcasted_iota(jnp.int32, (tokens, tokens), 1)
    tri = jnp.where(span_row >= span_col, 1.0, 0.0).astype(BF16)
    dot = functools.partial(jnp.dot, preferred_element_type=F32)

    def dot_t(a, b):
        return lax.dot_general(a, b, (((1,), (1,)), ((), ())), preferred_element_type=F32)

    cuts = [0] + [int(len(events) * (PRE + (SHARE - PRE) * k / (n_sp - 1))) for k in range(n_sp)]
    inside = cuts[-1]

    def block(k, carry):
        for i in range(n_sp):
            if cuts[i] < cuts[i + 1]:
                @pl.when(k == i)
                def _():
                    for event in events[cuts[i]:cuts[i + 1]]:
                        forward(*event)

        @pl.when(k != me)
        def _():
            chunk_copy(tx.at[me], rx.at[k], xsend.at[0], xrecv.at[k], me).wait_recv()

        before_re, before_im = carry
        br, bi, gr, gi, cr, ci = [bars[j, pl.ds(k, 1), :] for j in range(6)]
        chunk = rx[k]
        drive_re = (cr * inm[0] - ci * inm[1]).astype(BF16)
        drive_im = (cr * inm[1] + ci * inm[0]).astype(BF16)
        zero = jnp.zeros_like(drive_re)

        def inject(drive):
            return jnp.concatenate(
                [dot(chunk, jnp.concatenate([drive if q == p else zero for q in range(fold)], axis=0))
                 for p in range(fold)], axis=0)

        up_re, up_im = powers(gr, gi, tokens)
        sum_re, sum_im = cmul(inject(drive_re), inject(drive_im), up_re, up_im)
        sum_re, sum_im = dot(tri, sum_re.astype(BF16)), dot(tri, sum_im.astype(BF16))
        first_re, first_im = cmul(br, bi, before_re, before_im)
        down_re, down_im = powers(br, bi, tokens)
        state_re, state_im = cmul(sum_re + first_re, sum_im + first_im, down_re, down_im)
        s_re, s_im = state_re.astype(BF16), state_im.astype(BF16)
        response = skips * chunk.astype(F32)
        for p in range(fold):
            lines = slice(p * rows, (p + 1) * rows)
            response = response + dot_t(s_re[lines], cmat[2 * p]) - dot_t(s_im[lines], cmat[2 * p + 1])
        atx[k] = gelu(response).astype(BF16)

        @pl.when(k != me)
        def _():
            chunk_copy(atx.at[k], arx.at[me], asend.at[0], arecv.at[0], k).start()

        return state_re[tokens - 1:], state_im[tokens - 1:]

    lax.fori_loop(0, n_sp, block, (row_of(init, 0, 0), row_of(init, 0, 1)))

    most = n_sp - 1

    def weight(t, x):
        found = []
        for i in range(n_sp):
            where = {"x": x, "c": i % nc, "z": i // (nc * ny), "y": (i // nc) % ny}
            found.append(bufs[t][where["c"] * half + index(where)])
        return jnp.concatenate(found, axis=0)

    def complete(t):
        if paired:
            across(t, bufs[t].at[pl.ds((1 - at["c"]) * half, half)]).wait_recv()
        else:
            every = bufs[t].at[pl.ds(0, n_sp * n_dp - 1)]
            pltpu.make_async_remote_copy(
                src_ref=every, dst_ref=every, send_sem=wsend.at[t], recv_sem=wrecv.at[t, 0],
                device_id=device(at), device_id_type=MESH).wait_recv()

    def activated():
        arx[me] = atx[me]
        chunk_copy(atx.at[pl.ds(0, most)], arx.at[pl.ds(0, most)], asend.at[0], arecv.at[0], me).wait_recv()
        tiles = []
        for tile in range(sig.shape[1] // LANES):
            chunks = [arx[tile * fold + j].astype(F32) for j in range(fold)]
            parts = []
            for p in range(fold):
                acc = chunks[p]
                for j in range(fold):
                    if j != p:
                        moved = pltpu.roll(chunks[j], ((j - p) * wd) % LANES, 1)
                        acc = jnp.where(part == j, moved, acc)
                parts.append(acc)
            tiles.append(jnp.concatenate(parts, axis=0))
        return jnp.concatenate(tiles, axis=1)

    rest = events[inside:]
    mixed = None
    for t in pieces:
        soon = t if t == 0 else t + AHEAD
        last = max((i for i, event in enumerate(rest) if event[0] <= soon), default=-1)
        for event in rest[:last + 1]:
            forward(*event)
        rest = rest[last + 1:]
        if t == 0:
            act = activated()
            complete(0)
            gate = jnp.concatenate([dot(act.astype(BF16), weight(0, x)) for x in range(n_dp)], axis=1)
            gated = act * jax.nn.sigmoid(gate + b_glu[...])
            scale = lax.rsqrt(jnp.mean(gated * gated, axis=-1, keepdims=True) + 1e-06)
            mixed = (gated * scale * g_mix[...]).astype(BF16)
        else:
            complete(t)
            for x in range(n_dp):
                cols = slice((x * CUTS + t - 1) * ocols, (x * CUTS + t) * ocols)
                out[:, cols] = dot(mixed, weight(t, x)).astype(BF16)

    chunk_copy(tx.at[pl.ds(0, most)], rx.at[pl.ds(0, most)], xsend.at[0], xrecv.at[0], me).wait_send()
    chunk_copy(atx.at[pl.ds(0, most)], arx.at[pl.ds(0, most)], asend.at[0], arecv.at[0], me).wait_send()

    def drained(t, count):
        sent = bufs[t].at[pl.ds(0, count)]
        pltpu.make_async_remote_copy(
            src_ref=sent, dst_ref=sent, send_sem=wsend.at[t], recv_sem=wrecv.at[t, 0],
            device_id=device(at), device_id_type=MESH).wait_send()

    for t in pieces:
        if paired:
            across(t, bufs[t].at[pl.ds(at["c"] * half, half)]).wait_send()
            for z in range(nz):
                pl.when(at["z"] == z)(lambda z=z: drained(t, sends(t, z)))
        else:
            drained(t, n_sp * n_dp - 1)


def per_device(
    signal, pace, log_step, a_real, a_imag, in_map, out_map, skip, init_state, w_glu, b_glu, g_mix, w_out
):
    n_sp, n_dp = lax.axis_size("sp"), lax.axis_size("dp")
    tokens, width = signal.shape[1], signal.shape[2]
    groups, entries = a_real.shape
    channels = width // (groups * n_sp)
    wd = groups * channels
    states = groups * entries
    fold = LANES // wd
    rows = tokens // fold
    assert signal.shape[0] == 1 and pace.shape[1] == n_sp and n_sp % 4 == 0
    dims = {"x": n_dp, "c": 2, "y": 2, "z": n_sp // 4}
    wrows = w_out.shape[0]
    gcols, ocols = w_glu.shape[1], w_out.shape[1] // CUTS
    slots = n_sp * n_dp
    marks = slots // 2 if n_dp == 2 else 1
    chunk = pltpu.VMEM((n_sp, rows, LANES), BF16)
    sem = pltpu.SemaphoreType.DMA
    operands = (
        signal[0], a_real, a_imag, init_state, in_map.transpose(0, 1, 3, 2), out_map, log_step.reshape(1, -1), pace,
        skip.reshape(1, -1), b_glu.reshape(1, -1), g_mix.reshape(1, -1))
    output = pl.pallas_call(
        functools.partial(kernel, dims, (n_sp, n_dp, tokens, wd, fold, rows, states)),
        out_shape=pltpu.VMEM((tokens, w_out.shape[1] * n_dp), BF16),
        in_specs=[pl.BlockSpec(memory_space=pltpu.HBM)] * (len(operands) + 2),
        out_specs=pl.BlockSpec(memory_space=pltpu.VMEM),
        scratch_shapes=[
            pltpu.VMEM((slots, wrows, gcols if t == 0 else ocols), BF16) for t in range(len(ORDERS))
        ] + [pltpu.VMEM(x.shape, x.dtype) for x in operands] + [chunk] * 4 + [
            pltpu.VMEM((6, n_sp, states), F32),
            pltpu.VMEM((2 * fold, LANES, states), BF16),
            pltpu.VMEM((2, wd, states), F32),
            pltpu.SemaphoreType.REGULAR((4,)), sem((len(ORDERS),)), sem((len(operands),)),
            sem((len(ORDERS),)), sem((len(ORDERS), marks)), sem((len(ORDERS),)), sem((len(ORDERS),)),
            sem((1,)), sem((n_sp,)), sem((1,)), sem((1,)),
        ],
        compiler_params=pltpu.CompilerParams(
            collective_id=0, has_side_effects=True, vmem_limit_bytes=VMEM_LIMIT),
    )(*operands, w_glu, w_out)
    return output[None]


def solution(mesh):
    in_specs = (
        P("dp", "sp", None),
        P("dp", None),
        P("sp"),
        P("sp", None),
        P("sp", None),
        P("sp", None, None, None),
        P("sp", None, None, None),
        P("sp"),
        P("dp", None, "sp", None),
        P("sp", "dp"),
        P(),
        P(),
        P("sp", "dp"),
    )
    out_specs = P("dp", "sp", None)
    return jax.shard_map(
        per_device, mesh=mesh, in_specs=in_specs, out_specs=out_specs, check_vma=False
    )
```

```python
import functools
import math

import jax
import jax.numpy as jnp
from jax import lax
from jax.experimental import pallas as pl
from jax.experimental.pallas import tpu as pltpu
from jax.sharding import PartitionSpec as P

F32 = jnp.float32
BF16 = jnp.bfloat16
MESH = pl.DeviceIdType.MESH
LANES = 128
ORDERS = (("z", "y", "x"), ("z", "y", "x"), ("x", "z", "y"), ("y", "z", "x"), ("z", "x", "y"))
CUTS = len(ORDERS) - 1
SHARE = 0.68
PRE = 0.32
EARLY = 0
TOGETHER = 4
LAGS = (0.0, 0.2, 0.4, 0.6, 0.8)
AHEAD = 4
VMEM_LIMIT = 56 * 1024 * 1024


def cmul(ar, ai, br, bi):
    return ar * br - ai * bi, ar * bi + ai * br


def powers(br, bi, count):
    row = lax.broadcasted_iota(jnp.int32, (8, br.shape[1]), 0)
    pr = jnp.ones((8, br.shape[1]), F32)
    pi = jnp.zeros((8, br.shape[1]), F32)
    sr, si = br, bi
    for bit in (1, 2, 4):
        qr, qi = cmul(pr, pi, sr, si)
        on = (row & bit) != 0
        pr, pi = jnp.where(on, qr, pr), jnp.where(on, qi, pi)
        sr, si = cmul(sr, si, sr, si)
    size = 8
    while size < count:
        qr, qi = cmul(pr, pi, sr, si)
        pr = jnp.concatenate([pr, qr], axis=0)
        pi = jnp.concatenate([pi, qi], axis=0)
        sr, si = cmul(sr, si, sr, si)
        size *= 2
    return pr, pi


def gelu(v):
    return 0.5 * v * (1.0 + jnp.tanh(math.sqrt(2.0 / math.pi) * (v + 0.044715 * (v * v * v))))


def kernel(
    dims, sizes,
    sig_hbm, a_real_hbm, a_imag_hbm, init_hbm, in_map_hbm, out_map_hbm, log_hbm, pace_hbm, skip_hbm, b_glu_hbm,
    g_mix_hbm, wg_hbm, wo_hbm, out,
    buf0, buf1, buf2, buf3, buf4, sig, a_real, a_imag, init, in_map, out_map, log_step, pace, skip, b_glu, g_mix,
    tx, rx, atx, arx, bars, cmat, inm,
    ready, lsem, isem, wsend, wrecv, ssend, srecv, xsend, xrecv, asend, arecv,
):
    n_sp, n_dp, tokens, wd, fold, rows, states = sizes
    bufs = (buf0, buf1, buf2, buf3, buf4)
    pieces = range(len(ORDERS))
    me = lax.axis_index("sp")
    mx = lax.axis_index("dp")
    nx, nc, ny, nz = dims["x"], dims["c"], dims["y"], dims["z"]
    paired = n_dp == 2
    half = nx * ny * nz
    at = {"x": mx, "c": lax.rem(me, nc), "y": lax.rem(me // nc, ny), "z": me // (nc * ny)}
    ocols = wo_hbm.shape[1] // CUTS

    def device(where):
        return {"sp": (where["z"] * ny + where["y"]) * nc + where["c"], "dp": where["x"]}

    def index(where):
        return (where["x"] * ny + where["y"]) * nz + where["z"]

    def slot(t, where):
        return bufs[t].at[where["c"] * half + index(where)]

    loads = [
        pltpu.make_async_copy(src, dst, isem.at[j]) for j, (src, dst) in enumerate((
            (sig_hbm, sig), (a_real_hbm, a_real), (a_imag_hbm, a_imag), (init_hbm, init), (in_map_hbm, in_map),
            (out_map_hbm, out_map), (log_hbm, log_step), (pace_hbm, pace), (skip_hbm, skip), (b_glu_hbm, b_glu),
            (g_mix_hbm, g_mix)))
    ]
    local = [pltpu.make_async_copy(wg_hbm, slot(0, at), lsem.at[0])]
    for t in range(CUTS):
        local.append(pltpu.make_async_copy(
            wo_hbm.at[:, pl.ds(t * ocols, ocols)], slot(t + 1, at), lsem.at[t + 1]))

    barrier = pltpu.get_barrier_semaphore()

    def guarded(cond, action):
        if cond is None:
            action()
        else:
            pl.when(cond)(action)

    def step(axis, way):
        n, i = dims[axis], at[axis]
        if n == 2:
            return dict(at, **{axis: 1 - i}), None
        return dict(at, **{axis: jnp.clip(i + way, 0, n - 1)}), (i < n - 1) if way == 1 else (i > 0)

    ways = [(axis, way) for axis in ("z", "y", "x", "c") for way in ((1,) if dims[axis] == 2 else (1, -1))]

    def tell(semaphore, axis, way):
        to, ok = step(axis, way)
        guarded(ok, lambda: pl.semaphore_signal(semaphore, 1, device_id=device(to), device_id_type=MESH))

    def hear(semaphore, axis, way):
        guarded(step(axis, way)[1], lambda: pl.semaphore_wait(semaphore, 1))

    def greet_all(d, carry):
        to = lax.rem(me * n_dp + mx + d, n_sp * n_dp)
        pl.semaphore_signal(barrier, 1, device_id={"sp": to // n_dp, "dp": lax.rem(to, n_dp)}, device_id_type=MESH)
        return carry

    if paired:
        for axis, way in ways:
            tell(barrier, axis, way)
    else:
        lax.fori_loop(1, n_sp * n_dp, greet_all, 0)

    for copy in loads[:1] + local + loads[1:]:
        copy.start()
    if paired:
        peers = [step(axis, way)[1] for axis, way in ways]
        pl.semaphore_wait(barrier, sum(1 if ok is None else jnp.where(ok, 1, 0) for ok in peers))
    else:
        pl.semaphore_wait(barrier, n_sp * n_dp - 1)

    def hop(t, where, to):
        return pltpu.make_async_remote_copy(
            src_ref=slot(t, where), dst_ref=slot(t, where), send_sem=wsend.at[t],
            recv_sem=wrecv.at[t, index(where)], device_id=device(to), device_id_type=MESH)

    def across(t, ref):
        return pltpu.make_async_remote_copy(
            src_ref=ref, dst_ref=ref, send_sem=ssend.at[t], recv_sem=srecv.at[t],
            device_id=device(dict(at, c=1 - at["c"])), device_id_type=MESH)

    def source(move):
        where, cond = dict(at), None
        for axis, m in move.items():
            n, i = dims[axis], at[axis]
            if n == 2:
                where[axis] = 1 - i if m else i
            elif m:
                here = jnp.logical_and(i - m >= 0, i - m < n)
                cond = here if cond is None else jnp.logical_and(cond, here)
                where[axis] = jnp.clip(i - m, 0, n - 1)
        return where, cond

    def onward(order, move, level):
        found = []
        for deeper in range(level, len(order)):
            axis = order[deeper]
            n, m = dims[axis], move[axis]
            if n == 2:
                ways = () if m else (1,)
            else:
                ways = (1, -1) if m == 0 else ((m // abs(m),) if abs(m) < n - 1 else ())
            found += [(axis, way, deeper) for way in ways]
        return found

    def forward(t, move, level, first=False):
        where, cond = source(move)

        def act():
            if not first:
                hop(t, where, at).wait_recv()
            for axis, way, _ in onward(ORDERS[t], move, level):
                n, i = dims[axis], at[axis]
                if n == 2:
                    hop(t, where, dict(at, **{axis: 1 - i})).start()
                else:
                    ok = (i < n - 1) if way == 1 else (i > 0)
                    to = dict(at, **{axis: jnp.clip(i + way, 0, n - 1)})
                    pl.when(ok)(lambda to=to: hop(t, where, to).start())
            across(t, slot(t, where)).start()

        guarded(cond, act)

    def sends(t, z):
        total, wave = 0, [({axis: 0 for axis in ORDERS[t]}, 0)]
        while wave:
            later = []
            for move, level in wave:
                valid = 0 <= z - move["z"] < nz
                for axis, way, deeper in onward(ORDERS[t], move, level):
                    total += valid and (axis != "z" or 0 <= z + way < nz)
                    later.append((dict(move, **{axis: move[axis] + way}), deeper))
            wave = later
        return total

    def plan():
        waves, current = [], [(t, {axis: 0 for axis in ORDERS[t]}, 0) for t in pieces]
        depth = 0
        while current:
            later = []
            for t, move, level in current:
                for axis, way, deeper in onward(ORDERS[t], move, level):
                    later.append((t, dict(move, **{axis: move[axis] + way}), deeper))
            waves += [(depth + LAGS[event[0]], event) for event in later]
            current, depth = later, depth + 1
        return [event for _, event in sorted(waves, key=lambda found: found[0])]

    def toss(t, d):
        to = lax.rem(me * n_dp + mx + d, n_sp * n_dp)
        return pltpu.make_async_remote_copy(
            src_ref=slot(t, at), dst_ref=slot(t, at), send_sem=wsend.at[t], recv_sem=wrecv.at[t, 0],
            device_id={"sp": to // n_dp, "dp": lax.rem(to, n_dp)}, device_id_type=MESH)

    for copy in local:
        copy.wait()
    events = []
    if paired:
        events = plan()
        for t in pieces:
            forward(t, {axis: 0 for axis in ORDERS[t]}, 0, True)
    else:
        for t in pieces:
            def toss_one(d, carry, t=t):
                toss(t, d).start()
                return carry

            lax.fori_loop(1, n_sp * n_dp, toss_one, 0)

    loads[0].wait()
    part = lax.broadcasted_iota(jnp.int32, (rows, LANES), 1) // wd
    for tile in range(sig.shape[1] // LANES):
        cut = [
            sig[p * rows:(p + 1) * rows, tile * LANES:(tile + 1) * LANES].astype(F32) for p in range(fold)
        ]
        for j in range(fold):
            acc = cut[j]
            for p in range(fold):
                if p != j:
                    moved = pltpu.roll(cut[p], ((p - j) * wd) % LANES, 1)
                    acc = jnp.where(part == p, moved, acc)
            tx[tile * fold + j] = acc.astype(BF16)

    if paired:
        if dims["z"] > 2:
            for way in (1, -1):
                if way == -1:
                    for event in events[:EARLY]:
                        forward(*event)
                hear(ready.at[0 if way == 1 else 1], "z", -way)
                tell(ready.at[0 if way == 1 else 1], "z", way)
        else:
            tell(ready.at[0], "z", 1)
            hear(ready.at[0], "z", 1)
        for j, axis in ((2, "y"), (3, "c")):
            tell(ready.at[j], axis, 1)
            hear(ready.at[j], axis, 1)

    def chunk_copy(src, dst, ssem, rsem, to):
        return pltpu.make_async_remote_copy(
            src_ref=src, dst_ref=dst, send_sem=ssem, recv_sem=rsem,
            device_id={"sp": to, "dp": mx}, device_id_type=MESH)

    def send_chunk(d, carry):
        to = lax.rem(me + d, n_sp)
        chunk_copy(tx.at[to], rx.at[me], xsend.at[0], xrecv.at[me], to).start()
        return carry

    lax.fori_loop(1, n_sp, send_chunk, 0)

    for copy in loads[1:]:
        copy.wait()
    groups, entries = a_real.shape
    channels = wd // groups
    lane_group = lax.broadcasted_iota(jnp.int32, (1, states), 1) // entries

    def row_of(ref, *lead):
        found = [ref[lead + (slice(g, g + 1), slice(None))] for g in range(groups)]
        return jnp.concatenate(found, axis=1)

    a_re, a_im = row_of(a_real), row_of(a_imag)
    logs = log_step[...]
    log_row = jnp.broadcast_to(logs[:, :1], (1, states))
    for g in range(1, groups):
        log_row = jnp.where(lane_group == g, jnp.broadcast_to(logs[:, g:g + 1], (1, states)), log_row)
    on = lax.broadcasted_iota(jnp.int32, (n_sp, n_sp), 0) == lax.broadcasted_iota(jnp.int32, (n_sp, n_sp), 1)
    paces = jnp.sum(jnp.where(on, jnp.broadcast_to(pace[...], (n_sp, n_sp)), 0.0), axis=1, keepdims=True)
    steps = paces * jnp.exp(log_row)

    def diagonal(blocks):
        lines = []
        for g in range(groups):
            line = [jnp.zeros((channels, entries), F32)] * groups
            line[g] = blocks[g]
            lines.append(jnp.concatenate(line, axis=1))
        return jnp.concatenate(lines, axis=0)

    for j in range(2):
        inm[j] = diagonal([in_map[g, j] for g in range(groups)])
    skips = jnp.concatenate([skip[...]] * fold, axis=1)
    real, angle = a_re * steps, a_im * steps
    decay, growth = jnp.exp(real), jnp.exp(-real)
    cos, sin = jnp.cos(angle), jnp.sin(angle)
    bar_re, bar_im = decay * cos, decay * sin
    modulus = a_re * a_re + a_im * a_im
    bars[0] = bar_re
    bars[1] = bar_im
    bars[2] = growth * cos
    bars[3] = -growth * sin
    bars[4] = ((bar_re - 1.0) * a_re + bar_im * a_im) / modulus
    bars[5] = (bar_im * a_re - (bar_re - 1.0) * a_im) / modulus
    for p in range(fold):
        for j in range(2):
            blank = [jnp.zeros((wd, states), BF16)] * fold
            blank[p] = diagonal([out_map[g, j] for g in range(groups)]).astype(BF16)
            cmat[2 * p + j] = jnp.concatenate(blank, axis=0)

    rx[me] = tx[me]

    span_row = lax.broadcasted_iota(jnp.int32, (tokens, tokens), 0)
    span_col = lax.broadcasted_iota(jnp.int32, (tokens, tokens), 1)
    tri = jnp.where(span_row >= span_col, 1.0, 0.0).astype(BF16)
    dot = functools.partial(jnp.dot, preferred_element_type=F32)

    def dot_t(a, b):
        return lax.dot_general(a, b, (((1,), (1,)), ((), ())), preferred_element_type=F32)

    cuts = [EARLY if paired else 0] + [int(len(events) * (PRE + (SHARE - PRE) * k / (n_sp - 1))) for k in range(n_sp)]
    cuts = [max(cuts[0], cut) for cut in cuts]
    inside = cuts[-1]

    def injected(k):
        gr, gi, cr, ci = [bars[j, pl.ds(k, 1), :] for j in range(2, 6)]
        chunk = rx[k]
        drive_re = (cr * inm[0] - ci * inm[1]).astype(BF16)
        drive_im = (cr * inm[1] + ci * inm[0]).astype(BF16)
        zero = jnp.zeros_like(drive_re)

        def inject(drive):
            return jnp.concatenate(
                [dot(chunk, jnp.concatenate([drive if q == p else zero for q in range(fold)], axis=0))
                 for p in range(fold)], axis=0)

        up_re, up_im = powers(gr, gi, tokens)
        sum_re, sum_im = cmul(inject(drive_re), inject(drive_im), up_re, up_im)
        return dot(tri, sum_re.astype(BF16)), dot(tri, sum_im.astype(BF16))

    def advanced(k, sums, carry):
        br, bi = bars[0, pl.ds(k, 1), :], bars[1, pl.ds(k, 1), :]
        first_re, first_im = cmul(br, bi, *carry)
        down_re, down_im = powers(br, bi, tokens)
        return cmul(sums[0] + first_re, sums[1] + first_im, down_re, down_im)

    def responded(k, state_re, state_im):
        s_re, s_im = state_re.astype(BF16), state_im.astype(BF16)
        response = skips * rx[k].astype(F32)
        for p in range(fold):
            lines = slice(p * rows, (p + 1) * rows)
            response = response + dot_t(s_re[lines], cmat[2 * p]) - dot_t(s_im[lines], cmat[2 * p + 1])
        atx[k] = gelu(response).astype(BF16)

    def blocks(i, carry):
        group = [i * TOGETHER + j for j in range(TOGETHER)]
        for lead in range(0, n_sp, TOGETHER):
            inner = events[cuts[lead]:cuts[lead + TOGETHER]]
            if inner:
                @pl.when(i == lead // TOGETHER)
                def _():
                    for event in inner:
                        forward(*event)

        for k in group:
            @pl.when(k != me)
            def _():
                chunk_copy(tx.at[me], rx.at[k], xsend.at[0], xrecv.at[k], me).wait_recv()

        sums = [injected(k) for k in group]
        states = []
        for k, found in zip(group, sums):
            states.append(advanced(k, found, carry))
            carry = tuple(part[tokens - 1:] for part in states[-1])
        for k, state in zip(group, states):
            responded(k, *state)
        for k in group:
            @pl.when(k != me)
            def _():
                chunk_copy(atx.at[k], arx.at[me], asend.at[0], arecv.at[0], k).start()

        return carry

    lax.fori_loop(0, n_sp // TOGETHER, blocks, (row_of(init, 0, 0), row_of(init, 0, 1)))

    most = n_sp - 1

    def weight(t, x):
        found = []
        for i in range(n_sp):
            where = {"x": x, "c": i % nc, "z": i // (nc * ny), "y": (i // nc) % ny}
            found.append(bufs[t][where["c"] * half + index(where)])
        return jnp.concatenate(found, axis=0)

    def complete(t):
        if paired:
            across(t, bufs[t].at[pl.ds((1 - at["c"]) * half, half)]).wait_recv()
        else:
            every = bufs[t].at[pl.ds(0, n_sp * n_dp - 1)]
            pltpu.make_async_remote_copy(
                src_ref=every, dst_ref=every, send_sem=wsend.at[t], recv_sem=wrecv.at[t, 0],
                device_id=device(at), device_id_type=MESH).wait_recv()

    def activated():
        arx[me] = atx[me]
        chunk_copy(atx.at[pl.ds(0, most)], arx.at[pl.ds(0, most)], asend.at[0], arecv.at[0], me).wait_recv()
        tiles = []
        for tile in range(sig.shape[1] // LANES):
            chunks = [arx[tile * fold + j].astype(F32) for j in range(fold)]
            parts = []
            for p in range(fold):
                acc = chunks[p]
                for j in range(fold):
                    if j != p:
                        moved = pltpu.roll(chunks[j], ((j - p) * wd) % LANES, 1)
                        acc = jnp.where(part == j, moved, acc)
                parts.append(acc)
            tiles.append(jnp.concatenate(parts, axis=0))
        return jnp.concatenate(tiles, axis=1)

    rest = events[inside:]
    mixed = None
    for t in pieces:
        soon = t if t == 0 else t + AHEAD
        last = max((i for i, event in enumerate(rest) if event[0] <= soon), default=-1)
        for event in rest[:last + 1]:
            forward(*event)
        rest = rest[last + 1:]
        if t == 0:
            act = activated()
            complete(0)
            gate = jnp.concatenate([dot(act.astype(BF16), weight(0, x)) for x in range(n_dp)], axis=1)
            gated = act * jax.nn.sigmoid(gate + b_glu[...])
            scale = lax.rsqrt(jnp.mean(gated * gated, axis=-1, keepdims=True) + 1e-06)
            mixed = (gated * scale * g_mix[...]).astype(BF16)
        else:
            complete(t)
            for x in range(n_dp):
                cols = slice((x * CUTS + t - 1) * ocols, (x * CUTS + t) * ocols)
                out[:, cols] = dot(mixed, weight(t, x)).astype(BF16)

    chunk_copy(tx.at[pl.ds(0, most)], rx.at[pl.ds(0, most)], xsend.at[0], xrecv.at[0], me).wait_send()
    chunk_copy(atx.at[pl.ds(0, most)], arx.at[pl.ds(0, most)], asend.at[0], arecv.at[0], me).wait_send()

    def drained(t, count):
        sent = bufs[t].at[pl.ds(0, count)]
        pltpu.make_async_remote_copy(
            src_ref=sent, dst_ref=sent, send_sem=wsend.at[t], recv_sem=wrecv.at[t, 0],
            device_id=device(at), device_id_type=MESH).wait_send()

    for t in pieces:
        if paired:
            across(t, bufs[t].at[pl.ds(at["c"] * half, half)]).wait_send()
            for z in range(nz):
                pl.when(at["z"] == z)(lambda z=z: drained(t, sends(t, z)))
        else:
            drained(t, n_sp * n_dp - 1)


def per_device(
    signal, pace, log_step, a_real, a_imag, in_map, out_map, skip, init_state, w_glu, b_glu, g_mix, w_out
):
    n_sp, n_dp = lax.axis_size("sp"), lax.axis_size("dp")
    tokens, width = signal.shape[1], signal.shape[2]
    groups, entries = a_real.shape
    channels = width // (groups * n_sp)
    wd = groups * channels
    states = groups * entries
    fold = LANES // wd
    rows = tokens // fold
    assert signal.shape[0] == 1 and pace.shape[1] == n_sp and n_sp % 4 == 0 and n_sp % TOGETHER == 0
    dims = {"x": n_dp, "c": 2, "y": 2, "z": n_sp // 4}
    wrows = w_out.shape[0]
    gcols, ocols = w_glu.shape[1], w_out.shape[1] // CUTS
    slots = n_sp * n_dp
    marks = slots // 2 if n_dp == 2 else 1
    chunk = pltpu.VMEM((n_sp, rows, LANES), BF16)
    sem = pltpu.SemaphoreType.DMA
    operands = (
        signal[0], a_real, a_imag, init_state, in_map.transpose(0, 1, 3, 2), out_map, log_step.reshape(1, -1), pace,
        skip.reshape(1, -1), b_glu.reshape(1, -1), g_mix.reshape(1, -1))
    output = pl.pallas_call(
        functools.partial(kernel, dims, (n_sp, n_dp, tokens, wd, fold, rows, states)),
        out_shape=pltpu.VMEM((tokens, w_out.shape[1] * n_dp), BF16),
        in_specs=[pl.BlockSpec(memory_space=pltpu.HBM)] * (len(operands) + 2),
        out_specs=pl.BlockSpec(memory_space=pltpu.VMEM),
        scratch_shapes=[
            pltpu.VMEM((slots, wrows, gcols if t == 0 else ocols), BF16) for t in range(len(ORDERS))
        ] + [pltpu.VMEM(x.shape, x.dtype) for x in operands] + [chunk] * 4 + [
            pltpu.VMEM((6, n_sp, states), F32),
            pltpu.VMEM((2 * fold, LANES, states), BF16),
            pltpu.VMEM((2, wd, states), F32),
            pltpu.SemaphoreType.REGULAR((4,)), sem((len(ORDERS),)), sem((len(operands),)),
            sem((len(ORDERS),)), sem((len(ORDERS), marks)), sem((len(ORDERS),)), sem((len(ORDERS),)),
            sem((1,)), sem((n_sp,)), sem((1,)), sem((1,)),
        ],
        compiler_params=pltpu.CompilerParams(
            collective_id=0, has_side_effects=True, vmem_limit_bytes=VMEM_LIMIT),
    )(*operands, w_glu, w_out)
    return output[None]


def solution(mesh):
    in_specs = (
        P("dp", "sp", None),
        P("dp", None),
        P("sp"),
        P("sp", None),
        P("sp", None),
        P("sp", None, None, None),
        P("sp", None, None, None),
        P("sp"),
        P("dp", None, "sp", None),
        P("sp", "dp"),
        P(),
        P(),
        P("sp", "dp"),
    )
    out_specs = P("dp", "sp", None)
    return jax.shard_map(
        per_device, mesh=mesh, in_specs=in_specs, out_specs=out_specs, check_vma=False
    )
```

```python
import functools
import math

import jax
import jax.numpy as jnp
from jax import lax
from jax.experimental import pallas as pl
from jax.experimental.pallas import tpu as pltpu
from jax.sharding import PartitionSpec as P

F32 = jnp.float32
BF16 = jnp.bfloat16
MESH = pl.DeviceIdType.MESH
LANES = 128
ORDERS = (("z", "y", "x"), ("z", "y", "x"), ("x", "z", "y"), ("y", "z", "x"), ("z", "x", "y"))
CUTS = len(ORDERS) - 1
SHARE = 0.68
PRE = 0.32
EARLY = 0
TOGETHER = 4
LAGS = (0.0, 0.2, 0.4, 0.6, 0.8)
AHEAD = 4
VMEM_LIMIT = 56 * 1024 * 1024


def cmul(ar, ai, br, bi):
    return ar * br - ai * bi, ar * bi + ai * br


def powers(br, bi, count):
    row = lax.broadcasted_iota(jnp.int32, (8, br.shape[1]), 0)
    pr = jnp.ones((8, br.shape[1]), F32)
    pi = jnp.zeros((8, br.shape[1]), F32)
    sr, si = br, bi
    for bit in (1, 2, 4):
        qr, qi = cmul(pr, pi, sr, si)
        on = (row & bit) != 0
        pr, pi = jnp.where(on, qr, pr), jnp.where(on, qi, pi)
        sr, si = cmul(sr, si, sr, si)
    size = 8
    while size < count:
        qr, qi = cmul(pr, pi, sr, si)
        pr = jnp.concatenate([pr, qr], axis=0)
        pi = jnp.concatenate([pi, qi], axis=0)
        sr, si = cmul(sr, si, sr, si)
        size *= 2
    return pr, pi


def gelu(v):
    return 0.5 * v * (1.0 + jnp.tanh(math.sqrt(2.0 / math.pi) * (v + 0.044715 * (v * v * v))))


def kernel(
    dims, sizes,
    sig_hbm, a_real_hbm, a_imag_hbm, init_hbm, in_map_hbm, out_map_hbm, log_hbm, pace_hbm, skip_hbm, b_glu_hbm,
    g_mix_hbm, wg_hbm, wo_hbm, out,
    buf0, buf1, buf2, buf3, buf4, sig, a_real, a_imag, init, in_map, out_map, log_step, pace, skip, b_glu, g_mix,
    tx, rx, atx, arx, bars, cmat, inm,
    ready, lsem, isem, wsend, wrecv, ssend, srecv, xsend, xrecv, asend, arecv,
):
    n_sp, n_dp, tokens, wd, fold, rows, states = sizes
    bufs = (buf0, buf1, buf2, buf3, buf4)
    pieces = range(len(ORDERS))
    me = lax.axis_index("sp")
    mx = lax.axis_index("dp")
    nx, nc, ny, nz = dims["x"], dims["c"], dims["y"], dims["z"]
    paired = n_dp == 2
    half = nx * ny * nz
    at = {"x": mx, "c": lax.rem(me, nc), "y": lax.rem(me // nc, ny), "z": me // (nc * ny)}
    ocols = wo_hbm.shape[1] // CUTS

    def device(where):
        return {"sp": (where["z"] * ny + where["y"]) * nc + where["c"], "dp": where["x"]}

    def index(where):
        return (where["x"] * ny + where["y"]) * nz + where["z"]

    def slot(t, where):
        return bufs[t].at[where["c"] * half + index(where)]

    loads = [
        pltpu.make_async_copy(src, dst, isem.at[j]) for j, (src, dst) in enumerate((
            (sig_hbm, sig), (a_real_hbm, a_real), (a_imag_hbm, a_imag), (init_hbm, init), (in_map_hbm, in_map),
            (out_map_hbm, out_map), (log_hbm, log_step), (pace_hbm, pace), (skip_hbm, skip), (b_glu_hbm, b_glu),
            (g_mix_hbm, g_mix)))
    ]
    local = [pltpu.make_async_copy(wg_hbm, slot(0, at), lsem.at[0])]
    for t in range(CUTS):
        local.append(pltpu.make_async_copy(
            wo_hbm.at[:, pl.ds(t * ocols, ocols)], slot(t + 1, at), lsem.at[t + 1]))

    barrier = pltpu.get_barrier_semaphore()

    def guarded(cond, action):
        if cond is None:
            action()
        else:
            pl.when(cond)(action)

    def step(axis, way):
        n, i = dims[axis], at[axis]
        if n == 2:
            return dict(at, **{axis: 1 - i}), None
        return dict(at, **{axis: jnp.clip(i + way, 0, n - 1)}), (i < n - 1) if way == 1 else (i > 0)

    ways = [(axis, way) for axis in ("z", "y", "x", "c") for way in ((1,) if dims[axis] == 2 else (1, -1))]

    def tell(semaphore, axis, way):
        to, ok = step(axis, way)
        guarded(ok, lambda: pl.semaphore_signal(semaphore, 1, device_id=device(to), device_id_type=MESH))

    def hear(semaphore, axis, way):
        guarded(step(axis, way)[1], lambda: pl.semaphore_wait(semaphore, 1))

    def greet_all(d, carry):
        to = lax.rem(me * n_dp + mx + d, n_sp * n_dp)
        pl.semaphore_signal(barrier, 1, device_id={"sp": to // n_dp, "dp": lax.rem(to, n_dp)}, device_id_type=MESH)
        return carry

    if paired:
        for axis, way in ways:
            tell(barrier, axis, way)
    else:
        lax.fori_loop(1, n_sp * n_dp, greet_all, 0)

    for copy in loads[:1] + local + loads[1:]:
        copy.start()
    if paired:
        peers = [step(axis, way)[1] for axis, way in ways]
        pl.semaphore_wait(barrier, sum(1 if ok is None else jnp.where(ok, 1, 0) for ok in peers))
    else:
        pl.semaphore_wait(barrier, n_sp * n_dp - 1)

    def hop(t, where, to):
        return pltpu.make_async_remote_copy(
            src_ref=slot(t, where), dst_ref=slot(t, where), send_sem=wsend.at[t],
            recv_sem=wrecv.at[t, index(where)], device_id=device(to), device_id_type=MESH)

    def across(t, ref):
        return pltpu.make_async_remote_copy(
            src_ref=ref, dst_ref=ref, send_sem=ssend.at[t], recv_sem=srecv.at[t],
            device_id=device(dict(at, c=1 - at["c"])), device_id_type=MESH)

    def source(move):
        where, cond = dict(at), None
        for axis, m in move.items():
            n, i = dims[axis], at[axis]
            if n == 2:
                where[axis] = 1 - i if m else i
            elif m:
                here = jnp.logical_and(i - m >= 0, i - m < n)
                cond = here if cond is None else jnp.logical_and(cond, here)
                where[axis] = jnp.clip(i - m, 0, n - 1)
        return where, cond

    def onward(order, move, level):
        found = []
        for deeper in range(level, len(order)):
            axis = order[deeper]
            n, m = dims[axis], move[axis]
            if n == 2:
                ways = () if m else (1,)
            else:
                ways = (1, -1) if m == 0 else ((m // abs(m),) if abs(m) < n - 1 else ())
            found += [(axis, way, deeper) for way in ways]
        return found

    def forward(t, move, level, first=False):
        where, cond = source(move)

        def act():
            if not first:
                hop(t, where, at).wait_recv()
            for axis, way, _ in onward(ORDERS[t], move, level):
                n, i = dims[axis], at[axis]
                if n == 2:
                    hop(t, where, dict(at, **{axis: 1 - i})).start()
                else:
                    ok = (i < n - 1) if way == 1 else (i > 0)
                    to = dict(at, **{axis: jnp.clip(i + way, 0, n - 1)})
                    pl.when(ok)(lambda to=to: hop(t, where, to).start())
            across(t, slot(t, where)).start()

        guarded(cond, act)

    def sends(t, z):
        total, wave = 0, [({axis: 0 for axis in ORDERS[t]}, 0)]
        while wave:
            later = []
            for move, level in wave:
                valid = 0 <= z - move["z"] < nz
                for axis, way, deeper in onward(ORDERS[t], move, level):
                    total += valid and (axis != "z" or 0 <= z + way < nz)
                    later.append((dict(move, **{axis: move[axis] + way}), deeper))
            wave = later
        return total

    def plan():
        waves, current = [], [(t, {axis: 0 for axis in ORDERS[t]}, 0) for t in pieces]
        depth = 0
        while current:
            later = []
            for t, move, level in current:
                for axis, way, deeper in onward(ORDERS[t], move, level):
                    later.append((t, dict(move, **{axis: move[axis] + way}), deeper))
            waves += [(depth + LAGS[event[0]], event) for event in later]
            current, depth = later, depth + 1
        return [event for _, event in sorted(waves, key=lambda found: found[0])]

    def toss(t, d):
        to = lax.rem(me * n_dp + mx + d, n_sp * n_dp)
        return pltpu.make_async_remote_copy(
            src_ref=slot(t, at), dst_ref=slot(t, at), send_sem=wsend.at[t], recv_sem=wrecv.at[t, 0],
            device_id={"sp": to // n_dp, "dp": lax.rem(to, n_dp)}, device_id_type=MESH)

    for copy in local:
        copy.wait()
    events = []
    if paired:
        events = plan()
        for t in pieces:
            forward(t, {axis: 0 for axis in ORDERS[t]}, 0, True)
    else:
        for t in pieces:
            def toss_one(d, carry, t=t):
                toss(t, d).start()
                return carry

            lax.fori_loop(1, n_sp * n_dp, toss_one, 0)

    loads[0].wait()
    part = lax.broadcasted_iota(jnp.int32, (rows, LANES), 1) // wd
    for tile in range(sig.shape[1] // LANES):
        cut = [
            sig[p * rows:(p + 1) * rows, tile * LANES:(tile + 1) * LANES].astype(F32) for p in range(fold)
        ]
        for j in range(fold):
            acc = cut[j]
            for p in range(fold):
                if p != j:
                    moved = pltpu.roll(cut[p], ((p - j) * wd) % LANES, 1)
                    acc = jnp.where(part == p, moved, acc)
            tx[tile * fold + j] = acc.astype(BF16)

    if paired:
        if dims["z"] > 2:
            for way in (1, -1):
                if way == -1:
                    for event in events[:EARLY]:
                        forward(*event)
                hear(ready.at[0 if way == 1 else 1], "z", -way)
                tell(ready.at[0 if way == 1 else 1], "z", way)
        else:
            tell(ready.at[0], "z", 1)
            hear(ready.at[0], "z", 1)
        for j, axis in ((2, "y"), (3, "c")):
            tell(ready.at[j], axis, 1)
            hear(ready.at[j], axis, 1)

    def chunk_copy(src, dst, ssem, rsem, to):
        return pltpu.make_async_remote_copy(
            src_ref=src, dst_ref=dst, send_sem=ssem, recv_sem=rsem,
            device_id={"sp": to, "dp": mx}, device_id_type=MESH)

    def send_chunk(d, carry):
        to = lax.rem(me + d, n_sp)
        chunk_copy(tx.at[to], rx.at[me], xsend.at[0], xrecv.at[me // TOGETHER], to).start()
        return carry

    lax.fori_loop(1, n_sp, send_chunk, 0)

    for copy in loads[1:]:
        copy.wait()
    groups, entries = a_real.shape
    channels = wd // groups
    lane_group = lax.broadcasted_iota(jnp.int32, (1, states), 1) // entries

    def row_of(ref, *lead):
        found = [ref[lead + (slice(g, g + 1), slice(None))] for g in range(groups)]
        return jnp.concatenate(found, axis=1)

    a_re, a_im = row_of(a_real), row_of(a_imag)
    logs = log_step[...]
    log_row = jnp.broadcast_to(logs[:, :1], (1, states))
    for g in range(1, groups):
        log_row = jnp.where(lane_group == g, jnp.broadcast_to(logs[:, g:g + 1], (1, states)), log_row)
    on = lax.broadcasted_iota(jnp.int32, (n_sp, n_sp), 0) == lax.broadcasted_iota(jnp.int32, (n_sp, n_sp), 1)
    paces = jnp.sum(jnp.where(on, jnp.broadcast_to(pace[...], (n_sp, n_sp)), 0.0), axis=1, keepdims=True)
    steps = paces * jnp.exp(log_row)

    def diagonal(blocks):
        lines = []
        for g in range(groups):
            line = [jnp.zeros((channels, entries), F32)] * groups
            line[g] = blocks[g]
            lines.append(jnp.concatenate(line, axis=1))
        return jnp.concatenate(lines, axis=0)

    for j in range(2):
        inm[j] = diagonal([in_map[g, j] for g in range(groups)])
    skips = jnp.concatenate([skip[...]] * fold, axis=1)
    real, angle = a_re * steps, a_im * steps
    decay, growth = jnp.exp(real), jnp.exp(-real)
    cos, sin = jnp.cos(angle), jnp.sin(angle)
    bar_re, bar_im = decay * cos, decay * sin
    modulus = a_re * a_re + a_im * a_im
    bars[0] = bar_re
    bars[1] = bar_im
    bars[2] = growth * cos
    bars[3] = -growth * sin
    bars[4] = ((bar_re - 1.0) * a_re + bar_im * a_im) / modulus
    bars[5] = (bar_im * a_re - (bar_re - 1.0) * a_im) / modulus
    for p in range(fold):
        for j in range(2):
            blank = [jnp.zeros((wd, states), BF16)] * fold
            blank[p] = diagonal([out_map[g, j] for g in range(groups)]).astype(BF16)
            cmat[2 * p + j] = jnp.concatenate(blank, axis=0)

    rx[me] = tx[me]

    span_row = lax.broadcasted_iota(jnp.int32, (tokens, tokens), 0)
    span_col = lax.broadcasted_iota(jnp.int32, (tokens, tokens), 1)
    tri = jnp.where(span_row >= span_col, 1.0, 0.0).astype(BF16)
    dot = functools.partial(jnp.dot, preferred_element_type=F32)

    def dot_t(a, b):
        return lax.dot_general(a, b, (((1,), (1,)), ((), ())), preferred_element_type=F32)

    cuts = [EARLY if paired else 0] + [int(len(events) * (PRE + (SHARE - PRE) * k / (n_sp - 1))) for k in range(n_sp)]
    cuts = [max(cuts[0], cut) for cut in cuts]
    inside = cuts[-1]

    def injected(k):
        gr, gi, cr, ci = [bars[j, pl.ds(k, 1), :] for j in range(2, 6)]
        chunk = rx[k]
        drive_re = (cr * inm[0] - ci * inm[1]).astype(BF16)
        drive_im = (cr * inm[1] + ci * inm[0]).astype(BF16)
        zero = jnp.zeros_like(drive_re)

        def inject(drive):
            return jnp.concatenate(
                [dot(chunk, jnp.concatenate([drive if q == p else zero for q in range(fold)], axis=0))
                 for p in range(fold)], axis=0)

        up_re, up_im = powers(gr, gi, tokens)
        sum_re, sum_im = cmul(inject(drive_re), inject(drive_im), up_re, up_im)
        return dot(tri, sum_re.astype(BF16)), dot(tri, sum_im.astype(BF16))

    def advanced(k, sums, carry):
        br, bi = bars[0, pl.ds(k, 1), :], bars[1, pl.ds(k, 1), :]
        first_re, first_im = cmul(br, bi, *carry)
        down_re, down_im = powers(br, bi, tokens)
        return cmul(sums[0] + first_re, sums[1] + first_im, down_re, down_im)

    def responded(k, state_re, state_im):
        s_re, s_im = state_re.astype(BF16), state_im.astype(BF16)
        response = skips * rx[k].astype(F32)
        for p in range(fold):
            lines = slice(p * rows, (p + 1) * rows)
            response = response + dot_t(s_re[lines], cmat[2 * p]) - dot_t(s_im[lines], cmat[2 * p + 1])
        atx[k] = gelu(response).astype(BF16)

    def blocks(i, carry):
        group = [i * TOGETHER + j for j in range(TOGETHER)]
        for lead in range(0, n_sp, TOGETHER):
            inner = events[cuts[lead]:cuts[lead + TOGETHER]]
            if inner:
                @pl.when(i == lead // TOGETHER)
                def _():
                    for event in inner:
                        forward(*event)

        def await_chunks(count):
            some = rx.at[pl.ds(0, count)]
            chunk_copy(some, some, xsend.at[0], xrecv.at[i], me).wait_recv()

        mine = i == me // TOGETHER
        pl.when(jnp.logical_not(mine))(lambda: await_chunks(TOGETHER))
        if TOGETHER > 1:
            pl.when(mine)(lambda: await_chunks(TOGETHER - 1))

        sums = [injected(k) for k in group]
        states = []
        for k, found in zip(group, sums):
            states.append(advanced(k, found, carry))
            carry = tuple(part[tokens - 1:] for part in states[-1])
        for k, state in zip(group, states):
            responded(k, *state)
        for k in group:
            @pl.when(k != me)
            def _():
                chunk_copy(atx.at[k], arx.at[me], asend.at[0], arecv.at[0], k).start()

        return carry

    lax.fori_loop(0, n_sp // TOGETHER, blocks, (row_of(init, 0, 0), row_of(init, 0, 1)))

    most = n_sp - 1

    def weight(t, x):
        found = []
        for i in range(n_sp):
            where = {"x": x, "c": i % nc, "z": i // (nc * ny), "y": (i // nc) % ny}
            found.append(bufs[t][where["c"] * half + index(where)])
        return jnp.concatenate(found, axis=0)

    def complete(t):
        if paired:
            across(t, bufs[t].at[pl.ds((1 - at["c"]) * half, half)]).wait_recv()
        else:
            every = bufs[t].at[pl.ds(0, n_sp * n_dp - 1)]
            pltpu.make_async_remote_copy(
                src_ref=every, dst_ref=every, send_sem=wsend.at[t], recv_sem=wrecv.at[t, 0],
                device_id=device(at), device_id_type=MESH).wait_recv()

    def activated():
        arx[me] = atx[me]
        chunk_copy(atx.at[pl.ds(0, most)], arx.at[pl.ds(0, most)], asend.at[0], arecv.at[0], me).wait_recv()
        tiles = []
        for tile in range(sig.shape[1] // LANES):
            chunks = [arx[tile * fold + j].astype(F32) for j in range(fold)]
            parts = []
            for p in range(fold):
                acc = chunks[p]
                for j in range(fold):
                    if j != p:
                        moved = pltpu.roll(chunks[j], ((j - p) * wd) % LANES, 1)
                        acc = jnp.where(part == j, moved, acc)
                parts.append(acc)
            tiles.append(jnp.concatenate(parts, axis=0))
        return jnp.concatenate(tiles, axis=1)

    rest = events[inside:]
    mixed = None
    for t in pieces:
        soon = t if t == 0 else t + AHEAD
        last = max((i for i, event in enumerate(rest) if event[0] <= soon), default=-1)
        for event in rest[:last + 1]:
            forward(*event)
        rest = rest[last + 1:]
        if t == 0:
            act = activated()
            complete(0)
            gate = jnp.concatenate([dot(act.astype(BF16), weight(0, x)) for x in range(n_dp)], axis=1)
            gated = act * jax.nn.sigmoid(gate + b_glu[...])
            scale = lax.rsqrt(jnp.mean(gated * gated, axis=-1, keepdims=True) + 1e-06)
            mixed = (gated * scale * g_mix[...]).astype(BF16)
        else:
            complete(t)
            for x in range(n_dp):
                cols = slice((x * CUTS + t - 1) * ocols, (x * CUTS + t) * ocols)
                out[:, cols] = dot(mixed, weight(t, x)).astype(BF16)

    chunk_copy(tx.at[pl.ds(0, most)], rx.at[pl.ds(0, most)], xsend.at[0], xrecv.at[0], me).wait_send()
    chunk_copy(atx.at[pl.ds(0, most)], arx.at[pl.ds(0, most)], asend.at[0], arecv.at[0], me).wait_send()

    def drained(t, count):
        sent = bufs[t].at[pl.ds(0, count)]
        pltpu.make_async_remote_copy(
            src_ref=sent, dst_ref=sent, send_sem=wsend.at[t], recv_sem=wrecv.at[t, 0],
            device_id=device(at), device_id_type=MESH).wait_send()

    for t in pieces:
        if paired:
            across(t, bufs[t].at[pl.ds(at["c"] * half, half)]).wait_send()
            for z in range(nz):
                pl.when(at["z"] == z)(lambda z=z: drained(t, sends(t, z)))
        else:
            drained(t, n_sp * n_dp - 1)


def per_device(
    signal, pace, log_step, a_real, a_imag, in_map, out_map, skip, init_state, w_glu, b_glu, g_mix, w_out
):
    n_sp, n_dp = lax.axis_size("sp"), lax.axis_size("dp")
    tokens, width = signal.shape[1], signal.shape[2]
    groups, entries = a_real.shape
    channels = width // (groups * n_sp)
    wd = groups * channels
    states = groups * entries
    fold = LANES // wd
    rows = tokens // fold
    assert signal.shape[0] == 1 and pace.shape[1] == n_sp and n_sp % 4 == 0 and n_sp % TOGETHER == 0
    dims = {"x": n_dp, "c": 2, "y": 2, "z": n_sp // 4}
    wrows = w_out.shape[0]
    gcols, ocols = w_glu.shape[1], w_out.shape[1] // CUTS
    slots = n_sp * n_dp
    marks = slots // 2 if n_dp == 2 else 1
    chunk = pltpu.VMEM((n_sp, rows, LANES), BF16)
    sem = pltpu.SemaphoreType.DMA
    operands = (
        signal[0], a_real, a_imag, init_state, in_map.transpose(0, 1, 3, 2), out_map, log_step.reshape(1, -1), pace,
        skip.reshape(1, -1), b_glu.reshape(1, -1), g_mix.reshape(1, -1))
    output = pl.pallas_call(
        functools.partial(kernel, dims, (n_sp, n_dp, tokens, wd, fold, rows, states)),
        out_shape=pltpu.VMEM((tokens, w_out.shape[1] * n_dp), BF16),
        in_specs=[pl.BlockSpec(memory_space=pltpu.HBM)] * (len(operands) + 2),
        out_specs=pl.BlockSpec(memory_space=pltpu.VMEM),
        scratch_shapes=[
            pltpu.VMEM((slots, wrows, gcols if t == 0 else ocols), BF16) for t in range(len(ORDERS))
        ] + [pltpu.VMEM(x.shape, x.dtype) for x in operands] + [chunk] * 4 + [
            pltpu.VMEM((6, n_sp, states), F32),
            pltpu.VMEM((2 * fold, LANES, states), BF16),
            pltpu.VMEM((2, wd, states), F32),
            pltpu.SemaphoreType.REGULAR((4,)), sem((len(ORDERS),)), sem((len(operands),)),
            sem((len(ORDERS),)), sem((len(ORDERS), marks)), sem((len(ORDERS),)), sem((len(ORDERS),)),
            sem((1,)), sem((n_sp // TOGETHER,)), sem((1,)), sem((1,)),
        ],
        compiler_params=pltpu.CompilerParams(
            collective_id=0, has_side_effects=True, vmem_limit_bytes=VMEM_LIMIT),
    )(*operands, w_glu, w_out)
    return output[None]


def solution(mesh):
    in_specs = (
        P("dp", "sp", None),
        P("dp", None),
        P("sp"),
        P("sp", None),
        P("sp", None),
        P("sp", None, None, None),
        P("sp", None, None, None),
        P("sp"),
        P("dp", None, "sp", None),
        P("sp", "dp"),
        P(),
        P(),
        P("sp", "dp"),
    )
    out_specs = P("dp", "sp", None)
    return jax.shard_map(
        per_device, mesh=mesh, in_specs=in_specs, out_specs=out_specs, check_vma=False
    )
```
